128 devices in a mesh: sp: 16 (over z, x), dp: 8 (over y, core).
Axes of the slice: x: 4, y: 4, z: 4, core: 2. Of those that a mesh axis runs over, the one named last changes fastest.
Arguments:
- skip_stream_entering: bfloat16 [8, 2048, 2048], P('dp', 'sp'), may hold values from -6 to 6
- mapped_probe_matrix: bfloat16 [8, 2048, 2048], P('dp', 'sp'), may hold values from -6 to 6
- mapped_lookup_matrix: bfloat16 [8, 2048, 2048], P('dp', 'sp'), may hold values from -6 to 6
- mapped_content_matrix: bfloat16 [8, 2048, 4096], P('dp', 'sp'), may hold values from -6 to 6
- retention_preactivation: bfloat16 [8, 2048, 2048], P('dp', 'sp'), may hold values from -4 to 12
- extra_shrinkage: float32 [8, 16, 2048], P('dp', 'sp'), may hold values from -0.6932 to 0
- attention_group_scale: float32 [4096], replicated, may hold values from 0.1 to 1.9
- final_projection_matrix: bfloat16 [4096, 2048], P(None, 'dp'), may hold values from -0.09375 to 0.09375
- blender_branch_scale: float32 [2048], replicated, may hold values from 0.1 to 1.9
- specialist_prenormal_scale: float32 [2048], replicated, may hold values from 0.1 to 1.9
- specialist_switch_matrix: bfloat16 [128, 2048, 1024], P(('sp', 'dp')), may hold values from -0.125 to 0.125
- specialist_expand_matrix: bfloat16 [128, 2048, 1024], P(('sp', 'dp')), may hold values from -0.125 to 0.125
- specialist_contract_matrix: bfloat16 [128, 1024, 2048], P(('sp', 'dp')), may hold values from -0.1875 to 0.1875
- specialist_branch_scale: float32 [2048], replicated, may hold values from 0.1 to 1.9
- assigned_specialists: int32 [8, 2048, 2], P('dp', 'sp'), may hold values from 0 to 127, all different within a row; in each aligned block of 128 rows (0 to 127, 128 to 255, ..., all dimensions but the last counted through in order) at most 3 rows name the same one
- dispatcher_logits: float32 [8, 2048, 2], P('dp', 'sp'), may hold values from 0.2 to 1
Outputs:
- layer_out: bfloat16 [8, 2048, 2048], P('dp', 'sp')
The draws below stay inside these ranges and needn't reach their ends.
Inputs may be any that keep to these rules, and one draw needn't show every extreme that they name: `assigned_specialists`: in the rows of one device no expert is named more than 3 times; in every draw some expert reaches 3 on some device.
All inputs are finite; a program needn't handle non-finite values.
Results may differ from the reference program's by a relative error of at most 0.013.
Values may be sent and summed in bfloat16 or wider, within the bound.
A program may use at most 128 MiB of HBM per device.

```python
import math
import jax
import jax.numpy as jnp
import numpy as np
from jax import lax

D = 2048
ATTENTION_GROUPS = 16
KEY_WIDTH = 128
DV = 256
FF = 1024
TOP = 2
BLOCK = 64
TOK_DEV = 128
BATCH_SAMPLES = 8
TIME_STEPS = 2048
EXPERTS = 128
CAP = 3


def draw_retention_preactivation(key, part):
    kinds = jax.random.randint(jax.random.fold_in(key, 11), (ATTENTION_GROUPS,), 0, 10)
    slowness = (kinds >= 5).astype(jnp.float32)
    slow_center = math.log(TIME_STEPS / 24.0)
    centers = slowness * slow_center + (1.0 - slowness) * 0.5
    channel = jax.random.uniform(jax.random.fold_in(key, 12), (ATTENTION_GROUPS, KEY_WIDTH), jnp.float32, -0.5, 0.5)
    base_rate = (centers[:, None] + channel).reshape(ATTENTION_GROUPS * KEY_WIDTH)
    span_count = TIME_STEPS // TOK_DEV
    shifts = jax.random.uniform(jax.random.fold_in(key, 13), (BATCH_SAMPLES, span_count), jnp.float32, -0.7, 0.7)
    shifts = jnp.repeat(shifts, TOK_DEV, axis=1)
    jitter = 0.8 * jax.random.normal(jax.random.fold_in(key, 14), (BATCH_SAMPLES, TIME_STEPS, ATTENTION_GROUPS * KEY_WIDTH), jnp.float32)
    total = base_rate[None, None, :] + shifts[:, :, None] + jitter
    return jnp.clip(total, -4.0, 12.0).astype(jnp.bfloat16)


def draw_extra_shrinkage(key, part):
    spike_amount = 6
    timestep_offset = jax.random.randint(jax.random.fold_in(key, 21), (BATCH_SAMPLES, ATTENTION_GROUPS, spike_amount), 0, TIME_STEPS)
    tier_amount = jax.random.uniform(jax.random.fold_in(key, 22), (BATCH_SAMPLES, ATTENTION_GROUPS, spike_amount), jnp.float32, math.log(0.5), math.log(0.8))
    places = jnp.arange(TIME_STEPS, dtype=jnp.int32)
    matched = places[None, None, :, None] == timestep_offset[:, :, None, :]
    return jnp.min(jnp.where(matched, tier_amount[:, :, None, :], 0.0), axis=3)


def block_scale(key, dims, split, low, high):
    level = 1.0
    for dim, blocks in split:
        draws = jax.random.uniform(jax.random.fold_in(jax.random.fold_in(key, 6), dim), (blocks,), jnp.float32, low / len(split), high / len(split))
        level = level * jnp.repeat(jnp.exp(draws), dims[dim] // blocks).reshape((-1,) + (1,) * (len(dims) - 1 - dim))
    return level


def assign_block(stream_key, own, number, rows, number_of, top, bound, skew):
    order = jax.random.permutation(stream_key, number_of)
    packed, common = portions_of(number_of, rows * top, bound, skew, True), portions_of(number_of, rows * top, bound, skew, False)
    places = jnp.arange(number_of)

    def named(lengths, rotation):
        used = int((lengths > 0).sum())
        fixed = max(1, used // 4)
        shifted = fixed + (places - fixed + rotation * (used - fixed)) % max(1, number_of - fixed)
        return jnp.zeros((number_of,), jnp.int32).at[order[jnp.where(places < fixed, places, shifted)]].set(jnp.asarray(lengths, jnp.int32))

    lengths = jnp.where(number % 4 == 0, named(packed, number // 4), named(common, number - number // 4 - 1))
    mixed = jax.random.permutation(jax.random.fold_in(own, 3), number_of)
    donor, taker = mixed[0:number_of // 2 * 2:2], mixed[1:number_of // 2 * 2:2]
    room = jnp.minimum(lengths[donor] - 1, bound - lengths[taker]) // 2
    room = jnp.where((donor == order[0]) | (taker == order[0]) | (lengths[taker] == 0), 0, jnp.maximum(room, 0))
    shifted = jax.random.randint(jax.random.fold_in(own, 4), (number_of // 2,), 0, 1 << 20) % (room + 1)
    lengths = lengths.at[donor].add(-shifted).at[taker].add(shifted)
    members = jnp.searchsorted(jnp.cumsum(lengths), jnp.arange(rows * top), side="right").astype(jnp.int32)
    listing = members.reshape(top, rows).T
    listing = listing[jax.random.permutation(jax.random.fold_in(own, 1), rows)]
    rotation = jax.random.randint(jax.random.fold_in(own, 2), (rows, 1), 0, top)
    return jnp.take_along_axis(listing, (jnp.arange(top)[None, :] + rotation) % top, axis=1)


def portions_of(amount, total, bound, slope, full):
    weights = [(1 << 20) // math.isqrt(rank ** slope) + 1 for rank in range(1, amount + 1)]
    largest = bound if full else min(bound, max(-(-total // amount), total * weights[0] // sum(weights)))
    least = 1 if total - largest >= amount - 1 else 0
    holding, surplus = [largest] + [least] * (amount - 1), total - largest - least * (amount - 1)
    while surplus > 0:
        free = [i for i in range(1, amount) if holding[i] < largest] or [i for i in range(1, amount) if holding[i] < bound]
        whole, budget = sum([weights[i] for i in free]), surplus
        for i in free:
            extra = min(bound - holding[i], max(1, budget * weights[i] // whole), surplus)
            holding[i] = holding[i] + extra
            surplus = surplus - extra
    return np.array(holding)


def centred(own_key, shape, scale, limit, split=(), kind=jnp.bfloat16):
    drawn = jax.random.normal(own_key, shape, jnp.float32) * scale
    if len(split) > 0:
        drawn = block_scale(own_key, shape, split, -0.22, 0.18) * drawn
    return jnp.clip(drawn, min=-limit, max=limit).astype(kind)


def setup_inputs(seed: int = 0) -> dict:
    key_list = jax.random.split(jax.random.key(seed), 17)
    skip_stream_entering = centred(key_list[0], (BATCH_SAMPLES, TIME_STEPS, D), 1.0, 6.0, ((0, 8), (1, 16)))
    mapped_probe_matrix = centred(key_list[1], (BATCH_SAMPLES, TIME_STEPS, ATTENTION_GROUPS * KEY_WIDTH), 1.0, 6.0, ((0, 8), (1, 16)))
    mapped_lookup_matrix = centred(key_list[2], (BATCH_SAMPLES, TIME_STEPS, ATTENTION_GROUPS * KEY_WIDTH), 1.0, 6.0, ((0, 8), (1, 16)))
    mapped_content_matrix = centred(key_list[3], (BATCH_SAMPLES, TIME_STEPS, ATTENTION_GROUPS * DV), 1.0, 6.0, ((0, 8), (1, 16)))
    retention_preactivation = draw_retention_preactivation(jax.random.fold_in(key_list[16], 71), 0)
    extra_shrinkage = draw_extra_shrinkage(jax.random.fold_in(key_list[16], 71), 0)
    attention_group_scale = jnp.clip(1.0 + 0.18 * jax.random.normal(key_list[6], (ATTENTION_GROUPS * DV,), jnp.float32), 0.1, 1.9)
    final_projection_matrix = centred(key_list[7], (ATTENTION_GROUPS * DV, D), (ATTENTION_GROUPS * DV) ** -0.5, 0.09375, ((1, 8),))
    blender_branch_scale = jnp.clip(1.0 + 0.18 * jax.random.normal(key_list[8], (D,), jnp.float32), 0.1, 1.9)
    specialist_prenormal_scale = jnp.clip(1.0 + 0.18 * jax.random.normal(key_list[9], (D,), jnp.float32), 0.1, 1.9)
    specialist_switch_matrix = centred(key_list[10], (EXPERTS, D, FF), D ** -0.5, 0.125, ((0, 128),))
    specialist_expand_matrix = centred(key_list[11], (EXPERTS, D, FF), D ** -0.5, 0.125, ((0, 128),))
    specialist_contract_matrix = centred(key_list[12], (EXPERTS, FF, D), FF ** -0.5, 0.1875, ((0, 128),))
    specialist_branch_scale = jnp.clip(1.0 + 0.18 * jax.random.normal(key_list[13], (D,), jnp.float32), 0.1, 1.9)
    assigned_specialists_keys = jax.random.split(jax.random.fold_in(key_list[14], 1), BATCH_SAMPLES * TIME_STEPS // TOK_DEV)
    assigned_specialists_turns = jax.random.permutation(jax.random.fold_in(key_list[14], 3), BATCH_SAMPLES * TIME_STEPS // TOK_DEV)
    assigned_specialists = jax.vmap(lambda own, number: assign_block(jax.random.fold_in(key_list[14], 2), own, number, TOK_DEV, EXPERTS, TOP, CAP, 2))(assigned_specialists_keys, assigned_specialists_turns).reshape((BATCH_SAMPLES, TIME_STEPS, TOP))
    dispatcher_logits = jnp.clip(jnp.exp(math.log(1.0) - 1.609438 * jax.random.uniform(key_list[15], (BATCH_SAMPLES, TIME_STEPS, TOP), jnp.float32) ** block_scale(key_list[15], (BATCH_SAMPLES, TIME_STEPS, TOP), ((0, 8), (1, 16)), -0.2, 0.2)), 0.2, 1.0)
    return dict(skip_stream_entering=skip_stream_entering, mapped_probe_matrix=mapped_probe_matrix, mapped_lookup_matrix=mapped_lookup_matrix, mapped_content_matrix=mapped_content_matrix, retention_preactivation=retention_preactivation, extra_shrinkage=extra_shrinkage, attention_group_scale=attention_group_scale, final_projection_matrix=final_projection_matrix, blender_branch_scale=blender_branch_scale, specialist_prenormal_scale=specialist_prenormal_scale, specialist_switch_matrix=specialist_switch_matrix, specialist_expand_matrix=specialist_expand_matrix, specialist_contract_matrix=specialist_contract_matrix, specialist_branch_scale=specialist_branch_scale, assigned_specialists=assigned_specialists, dispatcher_logits=dispatcher_logits)


epsilon = 1e-06
softness_factor = 16.0
highest = lax.Precision.HIGHEST

def rms_scale(values, gain):
    mean_square = lax.optimization_barrier(jnp.mean(values * values, axis=-1, keepdims=True))
    return values * lax.rsqrt(mean_square + epsilon) * gain

def combine_states(earlier, later):
    return (earlier[0] * later[0], later[0][..., None] * earlier[1] + later[1])

def block_attention(query_f, key_f, value_f, shrink_exponent):
    length_value, head_count, key_dim = query_f.shape
    value_dim = value_f.shape[-1]
    block_count = length_value // BLOCK
    query_blocks = query_f.reshape(block_count, BLOCK, head_count, key_dim)
    key_blocks = key_f.reshape(block_count, BLOCK, head_count, key_dim)
    value_blocks = value_f.reshape(block_count, BLOCK, head_count, value_dim)
    within = jnp.cumsum(shrink_exponent.reshape(block_count, BLOCK, head_count, key_dim), axis=1)
    block_end = within[:, -1]
    lifted = query_blocks * jnp.exp(within)
    lowered = key_blocks * jnp.exp(-within)
    scores = jnp.einsum('nthk,nshk->nhts', lifted, lowered, precision=highest)
    causal = jnp.arange(BLOCK)[:, None] >= jnp.arange(BLOCK)[None, :]
    scores = jnp.where(causal, scores, 0.0)
    inside = jnp.einsum('nhts,nshv->nthv', scores, value_blocks, precision=highest)
    carried_keys = key_blocks * jnp.exp(block_end[:, None] - within)
    updates = jnp.einsum('nshk,nshv->nhkv', carried_keys, value_blocks, precision=highest)
    decays = jnp.exp(block_end)
    total_decay, states = lax.associative_scan(combine_states, (decays, updates), axis=0)
    entering = jnp.concatenate([jnp.zeros_like(states[:1]), states[:-1]], axis=0)
    across = jnp.einsum('nthk,nhkv->nthv', lifted, entering, precision=highest)
    outputs = (inside + across).reshape(length_value, head_count, value_dim)
    offsets = jnp.cumsum(block_end, axis=0) - block_end
    reached = (query_blocks * jnp.exp(within + offsets[:, None])).reshape(length_value, head_count, key_dim)
    return (outputs, total_decay[-1], states[-1], reached)

def reference(skip_stream_entering, mapped_probe_matrix, mapped_lookup_matrix, mapped_content_matrix, retention_preactivation, extra_shrinkage, attention_group_scale, final_projection_matrix, blender_branch_scale, specialist_prenormal_scale, specialist_switch_matrix, specialist_expand_matrix, specialist_contract_matrix, specialist_branch_scale, assigned_specialists, dispatcher_logits):

    def lone_series(fragment_array):
        probe_series, lookup_series, content_series, shrink_series, spike_series = fragment_array
        length_value = probe_series.shape[0]
        query_f = probe_series.reshape(length_value, ATTENTION_GROUPS, KEY_WIDTH).astype(jnp.float32) * KEY_WIDTH ** (-0.5)
        key_f = lookup_series.reshape(length_value, ATTENTION_GROUPS, KEY_WIDTH).astype(jnp.float32)
        value_f = content_series.reshape(length_value, ATTENTION_GROUPS, DV).astype(jnp.float32)
        shrink_exponent = jax.nn.log_sigmoid(shrink_series.reshape(length_value, ATTENTION_GROUPS, KEY_WIDTH).astype(jnp.float32)) / softness_factor
        shrink_exponent = shrink_exponent + jnp.transpose(spike_series)[:, :, None]
        outputs = block_attention(query_f, key_f, value_f, shrink_exponent)[0]
        return rms_scale(outputs, attention_group_scale.reshape(ATTENTION_GROUPS, DV)).astype(jnp.bfloat16)
    attention_group_result = lax.map(lone_series, (mapped_probe_matrix, mapped_lookup_matrix, mapped_content_matrix, retention_preactivation, extra_shrinkage))
    token_count = BATCH_SAMPLES * TIME_STEPS
    attention_group_result = attention_group_result.reshape(token_count, ATTENTION_GROUPS * DV)
    projected = jnp.dot(attention_group_result, final_projection_matrix, preferred_element_type=jnp.float32).astype(jnp.bfloat16)
    stream = skip_stream_entering.reshape(token_count, D).astype(jnp.float32)
    residual = (stream + rms_scale(projected.astype(jnp.float32), blender_branch_scale)).astype(jnp.bfloat16)
    expert_in = rms_scale(residual.astype(jnp.float32), specialist_prenormal_scale).astype(jnp.bfloat16)
    block_total = token_count // TOK_DEV
    pair_dev = TOK_DEV * TOP
    pair_count = token_count * TOP
    chosen = assigned_specialists.reshape(block_total, pair_dev)
    onehot = (chosen[:, :, None] == jnp.arange(EXPERTS, dtype=jnp.int32)[None, None, :]).astype(jnp.int32)
    ranks = lax.optimization_barrier(jnp.sum((jnp.cumsum(onehot, axis=1) - onehot) * onehot, axis=2))
    block_ids = jnp.arange(block_total, dtype=jnp.int32)[:, None]
    slots = (chosen * block_total + block_ids) * CAP + ranks
    pair_ids = jnp.arange(pair_count, dtype=jnp.int32)
    table = jnp.full((EXPERTS * block_total * CAP,), pair_count, jnp.int32)
    table = table.at[slots.reshape(-1)].set(pair_ids).reshape(EXPERTS, block_total * CAP)
    padded = jnp.concatenate([expert_in, jnp.zeros((1, D), jnp.bfloat16)], axis=0)

    def expert_step(carry, fragment_array):
        sources, gate_weight, up_weight, down_weight = fragment_array
        row_block = padded[sources // TOP]
        gate_part = jnp.dot(row_block, gate_weight, preferred_element_type=jnp.float32)
        up_part = jnp.dot(row_block, up_weight, preferred_element_type=jnp.float32)
        hidden_units = (jax.nn.silu(gate_part) * up_part).astype(jnp.bfloat16)
        result = jnp.dot(hidden_units, down_weight, preferred_element_type=jnp.float32).astype(jnp.bfloat16)
        return (carry.at[sources].set(result, mode='drop'), None)
    pair_out, _ = lax.scan(expert_step, jnp.zeros((pair_count, D), jnp.bfloat16), (table, specialist_switch_matrix, specialist_expand_matrix, specialist_contract_matrix))
    weights = dispatcher_logits.reshape(token_count, TOP)
    weights = weights / lax.optimization_barrier(jnp.sum(weights, axis=1, keepdims=True))
    combined = lax.optimization_barrier(jnp.sum(pair_out.reshape(token_count, TOP, D).astype(jnp.float32) * weights[:, :, None], axis=1))
    layer_out = residual.astype(jnp.float32) + rms_scale(combined, specialist_branch_scale)
    return layer_out.astype(jnp.bfloat16).reshape(BATCH_SAMPLES, TIME_STEPS, D)
```

```python
import functools
import jax
import jax.numpy as jnp
from jax import lax
from jax.experimental import pallas as pl
from jax.experimental.pallas import tpu as pltpu
from jax.sharding import PartitionSpec as P

MESH = pl.DeviceIdType.MESH
D = 2048
HEADS = 16
KW = 128
DV = 256
FF = 1024
TOK = 128
CAP = 3
EXPERTS = 128
PIECE = 512
HALF = 64
GROUPS = 2
PER = EXPERTS // GROUPS

epsilon = 1e-06
f32 = jnp.float32
bf16 = jnp.bfloat16


def dot_t(a, b, ca, cb):
    return lax.dot_general(a, b, (((ca,), (cb,)), ((), ())), preferred_element_type=f32)


def mixer_kernel(
    q_h, k_h, g_h, v_h, skip_h, spk, w_h, gs, bg, pg,
    res_out, x3_out,
    qv, kv, gv, vv, skipv, spk_in, wall,
    lf, lw, ca, lt, intra, us, ur, dsend, drecv, ss, sr, tall, pj, po, xf,
    lsem, spk_s, spk_r, w_s, w_r, u_s, u_r, d_s, d_r, s_s, s_r, t_s, t_r, p_s, p_r,
):
    sp = lax.axis_index("sp")
    dp = lax.axis_index("dp")
    z, x = sp // 4, sp % 4
    y, c = dp // 2, dp % 2
    partner = (sp, y * 2 + (1 - c))

    def remote(src, dst, s, r, dev):
        return pltpu.make_async_remote_copy(
            src_ref=src, dst_ref=dst, send_sem=s, recv_sem=r, device_id=dev, device_id_type=MESH
        )

    loads = [
        pltpu.make_async_copy(g_h, gv, lsem.at[0]),
        pltpu.make_async_copy(k_h, kv, lsem.at[1]),
        pltpu.make_async_copy(v_h, vv, lsem.at[2]),
        pltpu.make_async_copy(q_h, qv, lsem.at[3]),
        pltpu.make_async_copy(skip_h, skipv, lsem.at[4]),
        pltpu.make_async_copy(w_h, wall.at[0], lsem.at[5]),
    ]
    for one in loads:
        one.start()

    pltpu.make_async_copy(
        spk.at[:, pl.ds(pl.multiple_of(sp * TOK, TOK), TOK)], spk_in.at[sp], spk_r
    ).start()

    @pl.loop(1, HEADS)
    def _(i):
        to = (sp + i) % HEADS
        remote(
            spk.at[:, pl.ds(pl.multiple_of(to * TOK, TOK), TOK)], spk_in.at[sp], spk_s, spk_r, (to, dp)
        ).start()

    base = ((x + z) % 2) * 4
    obase = 4 - base
    up = (sp, ((y + 1) % 4) * 2 + c)
    down = (sp, ((y + 3) % 4) * 2 + c)
    around = [
        (z * 4 + (x + 1) % 4, dp),
        (z * 4 + (x + 3) % 4, dp),
        (((z + 1) % 4) * 4 + x, dp),
        (((z + 3) % 4) * 4 + x, dp),
    ]

    def rows(piece):
        return pl.ds(pl.multiple_of(piece * PIECE, PIECE), PIECE)

    for i in range(4):
        a, b = base + i, base + (i + 2) % 4
        remote(w_h.at[rows(a)], wall.at[1, rows(a)], w_s, w_r.at[0, a], up).start()
        remote(w_h.at[rows(b)], wall.at[3, rows(b)], w_s, w_r.at[2, b], down).start()

    def w_wait(slot, piece):
        there = wall.at[slot, rows(piece)]
        remote(there, there, w_s, w_r.at[slot - 1, piece], partner).wait_recv()

    def w_pass(slot, i):
        piece = base + i
        w_wait(slot, piece)
        there = wall.at[slot, rows(piece)]
        if slot == 1 and i < 2:
            remote(there, wall.at[2, rows(piece)], w_s, w_r.at[1, piece], up).start()
        if slot == 3 and i >= 2:
            remote(there, wall.at[2, rows(piece)], w_s, w_r.at[1, piece], down).start()
        remote(there, there, w_s, w_r.at[slot - 1, piece], around[i]).start()

    row = lax.broadcasted_iota(jnp.int32, (TOK, TOK), 0)
    col = lax.broadcasted_iota(jnp.int32, (TOK, TOK), 1)
    same = (row >= col) & ((row >= HALF) == (col >= HALF))
    cross = (row >= HALF) & (col < HALF)
    first = row < HALF
    tri = jnp.where(same, 1.0, 0.0).astype(bf16)

    for one in loads[:4]:
        one.wait()
    remote(spk_in.at[pl.ds(0, HEADS)], spk_in.at[pl.ds(0, HEADS)], spk_s, spk_r, partner).wait_recv()

    def u_send(h, part):
        rows_u = pl.ds(part * TOK, TOK)
        remote(us.at[h, rows_u], ur.at[sp, rows_u], u_s, u_r.at[part, sp], (h, dp)).start()

    @pl.loop(0, HEADS)
    def _(i):
        h = (sp + 1 + i) % HEADS
        lanes = pl.ds(pl.multiple_of(h * KW, KW), KW)
        g = gv[:, lanes].astype(f32)
        ld = (jnp.minimum(g, 0.0) - jnp.log1p(jnp.exp(-jnp.abs(g)))) * (1.0 / 16.0)
        ld = ld + jnp.broadcast_to(spk_in[h], (TOK, TOK)).T
        hi = ld.astype(bf16)
        rest = ld - hi.astype(f32)
        mid = rest.astype(bf16)
        low = (rest - mid.astype(f32)).astype(bf16)
        b = dot_t(tri, hi, 1, 0) + dot_t(tri, mid, 1, 0) + dot_t(tri, low, 1, 0)
        e1, e2 = b[HALF - 1 : HALF, :], b[TOK - 1 : TOK, :]
        kf = kv[:, lanes].astype(f32)
        qf = qv[:, lanes].astype(f32) * KW ** (-0.5)
        lifted = qf * jnp.exp(b)
        carried = kf * jnp.exp(jnp.where(first, e1, e2) - b)
        ku = carried * jnp.where(first, jnp.exp(e2), 1.0)
        vh = vv[:, pl.ds(pl.multiple_of(h * DV, DV), DV)]
        us[h] = dot_t(vh, ku.astype(bf16), 0, 0).astype(bf16)
        dsend[h] = jnp.exp(e1 + e2)
        lf[h] = lifted.astype(bf16)
        lw[h] = (kf * jnp.exp(-b)).astype(bf16)
        ca[h] = carried.astype(bf16)
        lt[h] = (lifted * jnp.where(first, 1.0, jnp.exp(e1))).astype(bf16)

        @pl.when(i > 0)
        def _():
            u_send((sp + i) % HEADS, 0)

    for part in range(2):
        rows_u = pl.ds(part * TOK, TOK)
        pltpu.make_async_copy(us.at[sp, rows_u], ur.at[sp, rows_u], u_r.at[part, sp]).start()
    pltpu.make_async_copy(dsend.at[sp], drecv.at[sp], d_r).start()

    @pl.loop(1, HEADS)
    def _(i):
        h = (sp + i) % HEADS
        remote(dsend.at[h], drecv.at[sp], d_s, d_r, (h, dp)).start()

    @pl.loop(1, HEADS)
    def _(i):
        u_send((sp + i) % HEADS, 1)

    w_pass(1, 0)
    w_pass(3, 2)

    @pl.loop(0, HEADS)
    def _(h):
        vh = vv[:, pl.ds(pl.multiple_of(h * DV, DV), DV)]
        near = dot_t(lf[h], lw[h], 1, 1)
        far = dot_t(lf[h], ca[h], 1, 1)
        scores = jnp.where(same, near, jnp.where(cross, far, 0.0))
        intra[h] = dot_t(scores.astype(bf16), vh, 1, 0)

    remote(drecv.at[pl.ds(0, HEADS)], drecv.at[pl.ds(0, HEADS)], d_s, d_r, partner).wait_recv()

    for part in range(2):
        rows_u = pl.ds(part * TOK, TOK)

        def step(src, state, rows_u=rows_u, part=part):
            ss[src, rows_u] = state.astype(bf16)

            @pl.when(src != sp)
            def _():
                remote(ss.at[src, rows_u], sr.at[sp, rows_u], s_s, s_r.at[part, sp], (src, dp)).start()

            @pl.when(src == sp)
            def _():
                pltpu.make_async_copy(ss.at[sp, rows_u], sr.at[sp, rows_u], s_r.at[part, sp]).start()

            there = ur.at[src, rows_u]
            remote(there, there, u_s, u_r.at[part, src], partner).wait_recv()
            return state * drecv[src] + ur[src, rows_u].astype(f32)

        lax.fori_loop(0, HEADS, step, jnp.zeros((TOK, KW), f32))
        w_pass(1, part + 1)
        w_pass(3, (part + 3) % 4)

    @pl.loop(0, HEADS)
    def _(i):
        h = (sp + i) % HEADS
        for part in range(2):
            there = sr.at[h, pl.ds(part * TOK, TOK)]
            remote(there, there, s_s, s_r.at[part, h], partner).wait_recv()
        o = intra[h] + dot_t(lt[h], sr[h], 1, 1)
        ms = jnp.mean(o * o, axis=-1, keepdims=True)
        lanes = pl.ds(pl.multiple_of(h * DV, DV), DV)
        tall[pl.ds(0, TOK), lanes] = (o * lax.rsqrt(ms + epsilon) * gs[:, lanes]).astype(bf16)

        @pl.when(i > 0)
        def _():
            prev = pl.ds(pl.multiple_of(((sp + i - 1) % HEADS) * DV, DV), DV)
            remote(tall.at[pl.ds(0, TOK), prev], tall.at[pl.ds(TOK, TOK), prev], t_s, t_r, partner).start()

    last = pl.ds(pl.multiple_of(((sp + HEADS - 1) % HEADS) * DV, DV), DV)
    w_pass(1, 3)
    w_pass(3, 1)
    remote(tall.at[pl.ds(0, TOK), last], tall.at[pl.ds(TOK, TOK), last], t_s, t_r, partner).start()
    loads[4].wait()
    loads[5].wait()
    remote(tall.at[pl.ds(0, TOK)], tall.at[pl.ds(TOK, TOK)], t_s, t_r, partner).wait_recv()

    def project(slot):
        acc = jnp.dot(tall[...], wall[slot], preferred_element_type=f32).astype(bf16)
        shard = ((y + 4 - slot) % 4) * 2 + c
        po[slot] = acc[TOK:]
        pj[shard] = acc[:TOK]
        remote(po.at[slot], pj.at[shard], p_s, p_r, partner).start()

    project(0)
    w_pass(2, 0)
    w_pass(2, 2)
    for i in range(4):
        w_wait(1, obase + i)
    project(1)
    w_pass(2, 1)
    w_pass(2, 3)
    for i in range(4):
        w_wait(3, obase + i)
    project(3)
    for i in range(4):
        w_wait(2, obase + i)
    project(2)
    remote(po.at[pl.ds(0, 4)], pj.at[pl.ds(0, 4)], p_s, p_r, partner).wait_recv()

    total = jnp.zeros((TOK, 1), f32)
    for n in range(8):
        p = pj[n].astype(f32)
        total = total + jnp.sum(p * p, axis=-1, keepdims=True)
    r1 = lax.rsqrt(total * (1.0 / D) + epsilon)
    total = jnp.zeros((TOK, 1), f32)
    for n in range(8):
        lanes = pl.ds(n * 256, 256)
        res = (skipv[:, lanes].astype(f32) + pj[n].astype(f32) * r1 * bg[:, lanes]).astype(bf16)
        res_out[:, lanes] = res
        rf = res.astype(f32)
        total = total + jnp.sum(rf * rf, axis=-1, keepdims=True)
    r2 = lax.rsqrt(total * (1.0 / D) + epsilon)
    for j in range(16):
        lanes = pl.ds(j * 128, 128)
        xf[pl.ds(j, TOK, stride=16), :] = res_out[:, lanes].astype(f32) * r2 * pg[:, lanes]

    @pl.loop(0, 8)
    def _(i):
        at = pl.ds(pl.multiple_of(i * 256, 256), 256)
        x3_out[at, :] = xf[at, :].astype(bf16)

    fifteen = pl.ds(0, HEADS - 1)
    remote(spk_in.at[fifteen], spk_in.at[fifteen], spk_s, spk_r, partner).wait_send()
    remote(drecv.at[fifteen], drecv.at[fifteen], d_s, d_r, partner).wait_send()
    remote(us.at[fifteen], ur.at[fifteen], u_s, u_r.at[0, 0], partner).wait_send()
    remote(ss.at[fifteen], sr.at[fifteen], s_s, s_r.at[0, 0], partner).wait_send()
    remote(tall.at[pl.ds(0, TOK)], tall.at[pl.ds(TOK, TOK)], t_s, t_r, partner).wait_send()
    remote(po.at[pl.ds(0, 4)], pj.at[pl.ds(0, 4)], p_s, p_r, partner).wait_send()
    remote(wall.at[pl.ds(0, 3)], wall.at[pl.ds(0, 3)], w_s, w_r.at[0, 0], partner).wait_send()


def mixer(q, k, g, v, skip, spk, w, gs, bg, pg):
    hbm = pl.BlockSpec(memory_space=pl.ANY)
    vmem = pl.BlockSpec(memory_space=pltpu.VMEM)
    dma = pltpu.SemaphoreType.DMA
    return pl.pallas_call(
        mixer_kernel,
        out_shape=(
            jax.ShapeDtypeStruct((TOK, D), bf16),
            jax.ShapeDtypeStruct((TOK * 16, 128), bf16),
        ),
        in_specs=[hbm] * 5 + [vmem, hbm, vmem, vmem, vmem],
        out_specs=(vmem, vmem),
        scratch_shapes=[
            pltpu.VMEM((TOK, D), bf16),
            pltpu.VMEM((TOK, D), bf16),
            pltpu.VMEM((TOK, D), bf16),
            pltpu.VMEM((TOK, HEADS * DV), bf16),
            pltpu.VMEM((TOK, D), bf16),
            pltpu.VMEM((HEADS, 1, TOK), f32),
            pltpu.VMEM((4, HEADS * DV, 256), bf16),
            pltpu.VMEM((HEADS, TOK, KW), bf16),
            pltpu.VMEM((HEADS, TOK, KW), bf16),
            pltpu.VMEM((HEADS, TOK, KW), bf16),
            pltpu.VMEM((HEADS, TOK, KW), bf16),
            pltpu.VMEM((HEADS, TOK, DV), f32),
            pltpu.VMEM((HEADS, DV, KW), bf16),
            pltpu.VMEM((HEADS, DV, KW), bf16),
            pltpu.VMEM((HEADS, 1, KW), f32),
            pltpu.VMEM((HEADS, 1, KW), f32),
            pltpu.VMEM((HEADS, DV, KW), bf16),
            pltpu.VMEM((HEADS, DV, KW), bf16),
            pltpu.VMEM((2 * TOK, HEADS * DV), bf16),
            pltpu.VMEM((8, TOK, 256), bf16),
            pltpu.VMEM((4, TOK, 256), bf16),
            pltpu.VMEM((TOK * 16, 128), f32),
            dma((6,)),
            dma, dma,
            dma, dma((3, 8)),
            dma, dma((2, HEADS)),
            dma, dma,
            dma, dma((2, HEADS)),
            dma, dma,
            dma, dma,
        ],
        compiler_params=pltpu.CompilerParams(has_side_effects=True, vmem_limit_bytes=56 * 2**20),
        name="mixer",
    )(q, k, g, v, skip, spk, w, gs, bg, pg)


def expert_kernel(
    tab, slots, wts, x3, res, gain, wg_h, wu_h, wd_h,
    out,
    xs, xr, ys, yr, rf, xm, hs, wg, wu, wd,
    wsem, x_s, x_r, y_s, y_r,
):
    sp = lax.axis_index("sp")
    dp = lax.axis_index("dp")
    z, x = sp // 4, sp % 4
    y, c = dp // 2, dp % 2

    def remote(src, dst, s, r, dev):
        return pltpu.make_async_remote_copy(
            src_ref=src, dst_ref=dst, send_sem=s, recv_sem=r, device_id=dev, device_id_type=MESH
        )

    def device(o, sign):
        oc, oz, ox, oy = o // 64, (o // 16) % 4, (o // 4) % 4, o % 4
        if sign < 0:
            oz, ox, oy = 4 - oz, 4 - ox, 4 - oy
        return (((z + oz) % 4) * 4 + (x + ox) % 4, ((y + oy) % 4) * 2 + (c + oc) % 2)

    partner = device(64, 1)
    loads = [
        pltpu.make_async_copy(wg_h, wg, wsem.at[0]),
        pltpu.make_async_copy(wu_h, wu, wsem.at[1]),
        pltpu.make_async_copy(wd_h, wd, wsem.at[2]),
    ]
    for one in loads:
        one.start()

    def pack(grp):
        @pl.loop(0, PER)
        def _(i):
            o = grp * PER + i
            for k in range(CAP):
                xs[o * CAP + k] = x3[tab[o * CAP + k]]

    def send(grp, src, dst, s, r, sign):
        if grp == 0:
            pltpu.make_async_copy(src.at[pl.ds(0, CAP)], dst.at[pl.ds(0, CAP)], r.at[0]).start()

        @pl.loop(1 if grp == 0 else 0, PER)
        def _(i):
            o = grp * PER + i
            at = pl.ds(o * CAP, CAP)
            remote(src.at[at], dst.at[at], s, r.at[grp], device(o, sign)).start()

    pack(0)
    send(0, xs, xr, x_s, x_r, 1)
    for grp in range(1, GROUPS):
        pack(grp)
        send(grp, xs, xr, x_s, x_r, 1)

    R = PER * CAP
    for grp in range(GROUPS):
        at = pl.ds(grp * R, R)
        remote(xr.at[at], xr.at[at], x_s, x_r.at[grp], partner).wait_recv()

        @pl.loop(0, R // 12)
        def _(i):
            rf[pl.ds(pl.multiple_of(i * 192, 192), 192), :] = (
                xr[pl.ds(grp * R + i * 12, 12)].astype(f32).reshape(192, 128)
            )

        for j in range(16):
            xm[:, pl.ds(j * 128, 128)] = rf[pl.ds(j, R, stride=16), :].astype(bf16)
        if grp == 0:
            loads[0].wait()
            loads[1].wait()

        @pl.loop(0, FF // 256)
        def _(n):
            lanes = pl.ds(pl.multiple_of(n * 256, 256), 256)
            a = jnp.dot(xm[...], wg[:, lanes], preferred_element_type=f32)
            b = jnp.dot(xm[...], wu[:, lanes], preferred_element_type=f32)
            hs[:, lanes] = (a * (1.0 / (1.0 + jnp.exp(-a))) * b).astype(bf16)

        if grp == 0:
            loads[2].wait()

        @pl.loop(0, D // 256)
        def _(n):
            lanes = pl.ds(pl.multiple_of(n * 256, 256), 256)
            a = jnp.dot(hs[...], wd[:, lanes], preferred_element_type=f32)
            rf[pl.ds(2 * n, R, stride=16), :] = a[:, :128]
            rf[pl.ds(2 * n + 1, R, stride=16), :] = a[:, 128:]

        @pl.loop(0, R // 12)
        def _(i):
            ys[pl.ds(grp * R + i * 12, 12)] = (
                rf[pl.ds(pl.multiple_of(i * 192, 192), 192), :].reshape(12, 16, 128).astype(bf16)
            )

        send(grp, ys, yr, y_s, y_r, -1)

    for grp in range(GROUPS):
        at = pl.ds(grp * R, R)
        remote(yr.at[at], yr.at[at], y_s, y_r.at[grp], partner).wait_recv()

    @pl.loop(0, TOK // 4)
    def _(i):
        for k in range(4):
            t = i * 4 + k
            one = yr[slots[2 * t]].astype(f32) * wts[2 * t]
            two = yr[slots[2 * t + 1]].astype(f32) * wts[2 * t + 1]
            rf[pl.ds(pl.multiple_of(t * 16, 16), 16), :] = one + two

    total = jnp.zeros((TOK, 1), f32)
    for j in range(16):
        p = rf[pl.ds(j, TOK, stride=16), :]
        total = total + jnp.sum(p * p, axis=-1, keepdims=True)
    r1 = lax.rsqrt(total * (1.0 / D) + epsilon)
    for j in range(16):
        lanes = pl.ds(j * 128, 128)
        p = rf[pl.ds(j, TOK, stride=16), :]
        out[:, lanes] = (res[:, lanes].astype(f32) + p * r1 * gain[:, lanes]).astype(bf16)

    most = pl.ds(0, (EXPERTS - 1) * CAP)
    remote(xs.at[most], xr.at[most], x_s, x_r.at[0], partner).wait_send()
    remote(ys.at[most], yr.at[most], y_s, y_r.at[0], partner).wait_send()


def experts(tab, slots, wts, x3, res, gain, wg, wu, wd):
    hbm = pl.BlockSpec(memory_space=pl.ANY)
    vmem = pl.BlockSpec(memory_space=pltpu.VMEM)
    smem = pl.BlockSpec(memory_space=pltpu.SMEM)
    dma = pltpu.SemaphoreType.DMA
    R = PER * CAP
    return pl.pallas_call(
        expert_kernel,
        out_shape=jax.ShapeDtypeStruct((TOK, D), bf16),
        in_specs=[smem] * 3 + [vmem] * 3 + [hbm] * 3,
        out_specs=vmem,
        scratch_shapes=[
            pltpu.VMEM((EXPERTS * CAP, 16, 128), bf16),
            pltpu.VMEM((EXPERTS * CAP, 16, 128), bf16),
            pltpu.VMEM((EXPERTS * CAP, 16, 128), bf16),
            pltpu.VMEM((EXPERTS * CAP, 16, 128), bf16),
            pltpu.VMEM((R * 16, 128), f32),
            pltpu.VMEM((R, D), bf16),
            pltpu.VMEM((R, FF), bf16),
            pltpu.VMEM((D, FF), bf16),
            pltpu.VMEM((D, FF), bf16),
            pltpu.VMEM((FF, D), bf16),
            dma((3,)),
            dma, dma((GROUPS,)),
            dma, dma((GROUPS,)),
        ],
        compiler_params=pltpu.CompilerParams(has_side_effects=True, vmem_limit_bytes=56 * 2**20),
        name="experts",
    )(tab, slots, wts, x3, res, gain, wg, wu, wd)


def routing(chosen, logits):
    sp = lax.axis_index("sp")
    dp = lax.axis_index("dp")
    z, x, y, c = sp // 4, sp % 4, dp // 2, dp % 2
    esp, edp = chosen // 8, chosen % 8
    o = (
        ((edp % 2 - c + 2) % 2) * 64
        + ((esp // 4 - z + 4) % 4) * 16
        + ((esp % 4 - x + 4) % 4) * 4
        + (edp // 2 - y + 4) % 4
    )
    lane = jnp.arange(EXPERTS, dtype=jnp.int32)
    pick = (o[:, :, None] == lane[None, None, :]).astype(f32)
    named = pick[:, 0] + pick[:, 1]
    time = jnp.arange(TOK, dtype=jnp.int32)
    before = (time[:, None] > time[None, :]).astype(bf16)
    rank = jnp.dot(before, named.astype(bf16), preferred_element_type=f32)
    place = lane.astype(f32)[None, :] * CAP + rank
    slots = jnp.sum(pick * place[:, None, :], axis=-1).astype(jnp.int32).reshape(-1)
    filled = named[:, :, None] * (rank[:, :, None] == jnp.arange(CAP, dtype=f32)[None, None, :])
    tab = jnp.sum(filled * time.astype(f32)[:, None, None], axis=0).astype(jnp.int32).reshape(-1)
    wts = logits / jnp.sum(logits, axis=1, keepdims=True)
    return tab, slots, wts.reshape(-1)


def shards(
    skip_stream_entering,
    mapped_probe_matrix,
    mapped_lookup_matrix,
    mapped_content_matrix,
    retention_preactivation,
    extra_shrinkage,
    attention_group_scale,
    final_projection_matrix,
    blender_branch_scale,
    specialist_prenormal_scale,
    specialist_switch_matrix,
    specialist_expand_matrix,
    specialist_contract_matrix,
    specialist_branch_scale,
    assigned_specialists,
    dispatcher_logits,
):
    tab, slots, wts = routing(assigned_specialists[0], dispatcher_logits[0])
    res, x3 = mixer(
        mapped_probe_matrix[0],
        mapped_lookup_matrix[0],
        retention_preactivation[0],
        mapped_content_matrix[0],
        skip_stream_entering[0],
        extra_shrinkage[0],
        final_projection_matrix,
        attention_group_scale.reshape(1, -1),
        blender_branch_scale.reshape(1, -1),
        specialist_prenormal_scale.reshape(1, -1),
    )
    out = experts(
        tab,
        slots,
        wts,
        x3.reshape(TOK, 16, 128),
        res,
        specialist_branch_scale.reshape(1, -1),
        specialist_switch_matrix[0],
        specialist_expand_matrix[0],
        specialist_contract_matrix[0],
    )
    return out[None]


def solution(mesh):
    return jax.shard_map(
        shards,
        mesh=mesh,
        in_specs=(
            P("dp", "sp", None),
            P("dp", "sp", None),
            P("dp", "sp", None),
            P("dp", "sp", None),
            P("dp", "sp", None),
            P("dp", "sp", None),
            P(),
            P(None, "dp"),
            P(),
            P(),
            P(("sp", "dp"), None, None),
            P(("sp", "dp"), None, None),
            P(("sp", "dp"), None, None),
            P(),
            P("dp", "sp", None),
            P("dp", "sp", None),
        ),
        out_specs=P("dp", "sp", None),
        check_vma=False,
    )
```

```python
import jax
import jax.numpy as jnp
from jax import lax
from jax.experimental import pallas as pl
from jax.experimental.pallas import tpu as pltpu
from jax.sharding import PartitionSpec as P

MESH = pl.DeviceIdType.MESH
D = 2048
HEADS = 16
KW = 128
DV = 256
FF = 1024
TOK = 128
TOP = 2
CAP = 3
EXPERTS = 128
PIECE = 512
HALF = 64
GROUPS = 2
PER = EXPERTS // GROUPS

epsilon = 1e-06
f32 = jnp.float32
bf16 = jnp.bfloat16


def dot_t(a, b, ca, cb):
    return lax.dot_general(a, b, (((ca,), (cb,)), ((), ())), preferred_element_type=f32)


def phases():
    held = []

    def begin(name):
        if held:
            held.pop().__exit__(None, None, None)
        if name:
            scope = jax.named_scope(name)
            scope.__enter__()
            held.append(scope)

    return begin


def layer_kernel(
    q_h, k_h, g_h, v_h, skip_h, spk, w_h, gs, bg, pg, chosen, logits, gain, wg_h, wu_h, wd_h,
    res_out, norm_out,
    qv, kv, gv, vv, skipv, spk_in, wall,
    bgs, lf, lw, ca, lt, intra, us, ur, dsend, drecv, ss, sr, tall, pj, po, rf,
    x3, xs, xr, ys, yr, xm, hs, wg, wu, wd, idx_v, wts_v, idx, wts,
    lsem, spk_s, spk_r, w_s, w_r, u_s, u_r, d_s, d_r, s_s, s_r, t_s, t_r, p_s, p_r,
    esem, isem, x_s, x_r, y_s, y_r,
):
    ph = phases()
    sp = lax.axis_index("sp")
    dp = lax.axis_index("dp")
    z, x = sp // 4, sp % 4
    y, c = dp // 2, dp % 2
    partner = (sp, y * 2 + (1 - c))
    dps = [[((y + dy) % 4) * 2 + (c + dc) % 2 for dc in range(2)] for dy in range(4)]

    def ahead(i):
        return ((z + i // 4) % 4) * 4 + (x + i % 4) % 4

    def behind(i):
        return ((z + 4 - i // 4) % 4) * 4 + (x + 4 - i % 4) % 4

    def remote(src, dst, s, r, dev):
        return pltpu.make_async_remote_copy(
            src_ref=src, dst_ref=dst, send_sem=s, recv_sem=r, device_id=dev, device_id_type=MESH
        )

    ph("m_start")
    loads = [
        pltpu.make_async_copy(g_h, gv, lsem.at[0]),
        pltpu.make_async_copy(k_h, kv, lsem.at[1]),
        pltpu.make_async_copy(v_h, vv, lsem.at[2]),
        pltpu.make_async_copy(q_h, qv, lsem.at[3]),
        pltpu.make_async_copy(skip_h, skipv, lsem.at[4]),
        pltpu.make_async_copy(w_h, wall.at[0], lsem.at[5]),
    ]
    for one in loads:
        one.start()

    barrier = pltpu.get_barrier_semaphore()

    def greet(to, skip):
        for dy in range(4):
            for dc in range(2):
                if not (skip and dy == 0 and dc == 0):
                    pl.semaphore_signal(
                        barrier, inc=1, device_id=(to, dps[dy][dc]), device_id_type=MESH
                    )

    greet(sp, True)

    @pl.loop(1, HEADS)
    def _(i):
        greet(ahead(i), False)

    row = lax.broadcasted_iota(jnp.int32, (TOK, TOK), 0)
    col = lax.broadcasted_iota(jnp.int32, (TOK, TOK), 1)
    same = (row >= col) & ((row >= HALF) == (col >= HALF))
    cross = (row >= HALF) & (col < HALF)
    first = row < HALF
    tri = jnp.where(same, 1.0, 0.0).astype(bf16)

    def split(a):
        hi = a.astype(bf16)
        rest = a - hi.astype(f32)
        mid = rest.astype(bf16)
        return hi, mid, (rest - mid.astype(f32)).astype(bf16)

    ph("m_decay")
    loads[0].wait()

    @pl.loop(0, HEADS // 2)
    def _(i):
        for k in range(2):
            h = i * 2 + k
            g = gv[:, pl.ds(pl.multiple_of(h * KW, KW), KW)].astype(f32)
            ld = (jnp.minimum(g, 0.0) - jnp.log1p(jnp.exp(-jnp.abs(g)))) * (1.0 / 16.0)
            hi, mid, low = split(ld)
            bgs[h] = dot_t(tri, hi, 1, 0) + dot_t(tri, mid, 1, 0) + dot_t(tri, low, 1, 0)

    ph("m_barrier")
    pl.semaphore_wait(barrier, EXPERTS - 1)
    ph("m_first")
    pltpu.make_async_copy(
        spk.at[:, pl.ds(pl.multiple_of(sp * TOK, TOK), TOK)], spk_in.at[sp], spk_r
    ).start()

    @pl.loop(1, HEADS)
    def _(i):
        to = (sp + i) % HEADS
        remote(
            spk.at[:, pl.ds(pl.multiple_of(to * TOK, TOK), TOK)], spk_in.at[sp], spk_s, spk_r, (to, dp)
        ).start()

    base = ((x + z) % 2) * 4
    obase = 4 - base
    up = (sp, dps[1][0])
    down = (sp, dps[3][0])
    around = [(ahead(1), dp), (ahead(3), dp), (ahead(4), dp), (ahead(12), dp)]

    def rows(piece):
        return pl.ds(pl.multiple_of(piece * PIECE, PIECE), PIECE)

    for i in range(4):
        a, b = base + i, base + (i + 2) % 4
        remote(w_h.at[rows(a)], wall.at[1, rows(a)], w_s, w_r.at[0, a], up).start()
        remote(w_h.at[rows(b)], wall.at[3, rows(b)], w_s, w_r.at[2, b], down).start()

    def w_wait(slot, piece):
        there = wall.at[slot, rows(piece)]
        remote(there, there, w_s, w_r.at[slot - 1, piece], partner).wait_recv()

    def w_pass(slot, i):
        piece = base + i
        w_wait(slot, piece)
        there = wall.at[slot, rows(piece)]
        if slot == 1 and i < 2:
            remote(there, wall.at[2, rows(piece)], w_s, w_r.at[1, piece], up).start()
        if slot == 3 and i >= 2:
            remote(there, wall.at[2, rows(piece)], w_s, w_r.at[1, piece], down).start()
        remote(there, there, w_s, w_r.at[slot - 1, piece], around[i]).start()

    ph("m_route")
    esp, edp = chosen[...] >> 3, chosen[...] & 7
    off = (
        (((edp & 1) + c) & 1) * 64
        + (((esp >> 2) + 4 - z) & 3) * 16
        + (((esp & 3) + 4 - x) & 3) * 4
        + (((edp >> 1) + 4 - y) & 3)
    )
    pick = [jnp.where(row == off[r : r + 1], 1.0, 0.0) for r in range(TOP)]
    named = pick[0] + pick[1]
    later = jnp.where(row < col, 1.0, 0.0).astype(bf16)
    rank = dot_t(named.astype(bf16), later, 1, 0)
    place = row.astype(f32) * CAP + rank
    idx_v[...] = jnp.zeros((8, TOK), jnp.int32)
    times = jnp.where(lax.broadcasted_iota(jnp.int32, (8, TOK), 0) >= 0, 1.0, 0.0) * (
        lax.broadcasted_iota(jnp.int32, (8, TOK), 1).astype(f32)
    )
    for k in range(CAP):
        filled = jnp.where(rank == float(k), named, 0.0).astype(bf16)
        found = dot_t(times.astype(bf16), filled, 1, 1)
        idx_v[k : k + 1, :] = jnp.minimum(found[:1], TOK - 1.0).astype(jnp.int32)
    for r in range(TOP):
        at = jnp.sum(pick[r] * place, axis=0, keepdims=True)
        idx_v[CAP + r : CAP + r + 1, :] = jnp.minimum(at, EXPERTS * CAP - 1.0).astype(jnp.int32)
    lg = logits[...]
    wts_v[...] = lg / (lg[0:1] + lg[1:2])
    tables = [
        pltpu.make_async_copy(idx_v, idx, isem.at[0]),
        pltpu.make_async_copy(wts_v, wts, isem.at[1]),
    ]

    ph("m_loadwait")
    for one in loads[1:4]:
        one.wait()
    remote(spk_in.at[pl.ds(0, HEADS)], spk_in.at[pl.ds(0, HEADS)], spk_s, spk_r, partner).wait_recv()
    ph("m_loopA")

    def u_send(h, part):
        rows_u = pl.ds(part * TOK, TOK)
        remote(us.at[h, rows_u], ur.at[sp, rows_u], u_s, u_r.at[part, sp], (h, dp)).start()

    def form(h):
        lanes = pl.ds(pl.multiple_of(h * KW, KW), KW)
        hi, mid, low = split(jnp.broadcast_to(spk_in[h], (TOK, TOK)).T)
        b = bgs[h] + dot_t(tri, hi, 1, 0) + dot_t(tri, mid, 1, 0) + dot_t(tri, low, 1, 0)
        e1, e2 = b[HALF - 1 : HALF, :], b[TOK - 1 : TOK, :]
        kf = kv[:, lanes].astype(f32)
        qf = qv[:, lanes].astype(f32) * KW ** (-0.5)
        carried = kf * jnp.exp(jnp.where(first, e1, e2) - b)
        ku = carried * jnp.where(first, jnp.exp(e2), 1.0)
        vh = vv[:, pl.ds(pl.multiple_of(h * DV, DV), DV)]
        us[h] = dot_t(vh, ku.astype(bf16), 0, 0).astype(bf16)
        dsend[h] = jnp.exp(e1 + e2)
        lifted = qf * jnp.exp(b)
        lf[h] = lifted.astype(bf16)
        lw[h] = (kf * jnp.exp(-b)).astype(bf16)
        ca[h] = carried.astype(bf16)
        lt[h] = (lifted * jnp.where(first, 1.0, jnp.exp(e1))).astype(bf16)

    @pl.loop(0, HEADS // 2)
    def _(i):
        for k in range(2):
            form((sp + 1 + 2 * i + k) % HEADS)

        u_send((sp + 1 + 2 * i) % HEADS, 0)

        @pl.when(i < HEADS // 2 - 1)
        def _():
            u_send((sp + 2 + 2 * i) % HEADS, 0)

    ph("m_sendB")
    for part in range(2):
        rows_u = pl.ds(part * TOK, TOK)
        pltpu.make_async_copy(us.at[sp, rows_u], ur.at[sp, rows_u], u_r.at[part, sp]).start()
    pltpu.make_async_copy(dsend.at[sp], drecv.at[sp], d_r).start()

    @pl.loop(1, HEADS)
    def _(i):
        h = (sp + i) % HEADS
        remote(dsend.at[h], drecv.at[sp], d_s, d_r, (h, dp)).start()

    @pl.loop(1, HEADS)
    def _(i):
        u_send((sp + i) % HEADS, 1)

    for one in tables:
        one.start()
    experts_in = [
        pltpu.make_async_copy(wg_h, wg, esem.at[0]),
        pltpu.make_async_copy(wu_h, wu, esem.at[1]),
        pltpu.make_async_copy(wd_h, wd, esem.at[2]),
    ]
    for one in experts_in:
        one.start()

    ph("m_loopB")

    @pl.loop(0, HEADS // 2)
    def _(i):
        for k in range(2):
            h = 2 * i + k
            vh = vv[:, pl.ds(pl.multiple_of(h * DV, DV), DV)]
            near = dot_t(lf[h], lw[h], 1, 1)
            far = dot_t(lf[h], ca[h], 1, 1)
            scores = jnp.where(same, near, jnp.where(cross, far, 0.0))
            intra[h] = dot_t(scores.astype(bf16), vh, 1, 0)

    ph("m_w0")
    w_pass(1, 0)
    w_pass(3, 2)
    ph("m_dwait")
    remote(drecv.at[pl.ds(0, HEADS)], drecv.at[pl.ds(0, HEADS)], d_s, d_r, partner).wait_recv()

    for part in range(2):
        ph(f"m_scan{part}")
        rows_u = pl.ds(part * TOK, TOK)

        def step(src, state, rows_u=rows_u, part=part):
            ss[src, rows_u] = state.astype(bf16)

            @pl.when(src != sp)
            def _():
                remote(ss.at[src, rows_u], sr.at[sp, rows_u], s_s, s_r.at[part, sp], (src, dp)).start()

            @pl.when(src == sp)
            def _():
                pltpu.make_async_copy(ss.at[sp, rows_u], sr.at[sp, rows_u], s_r.at[part, sp]).start()

            there = ur.at[src, rows_u]
            remote(there, there, u_s, u_r.at[part, src], partner).wait_recv()
            return state * drecv[src] + ur[src, rows_u].astype(f32)

        lax.fori_loop(0, HEADS, step, jnp.zeros((TOK, KW), f32))
        ph(f"m_w{part + 1}")
        w_pass(1, part + 1)
        w_pass(3, (part + 3) % 4)

    def attend(i):
        h = (sp + i) % HEADS
        for part in range(2):
            there = sr.at[h, pl.ds(part * TOK, TOK)]
            remote(there, there, s_s, s_r.at[part, h], partner).wait_recv()
        o = intra[h] + dot_t(lt[h], sr[h], 1, 1)
        ms = jnp.mean(o * o, axis=-1, keepdims=True)
        lanes = pl.ds(pl.multiple_of(h * DV, DV), DV)
        tall[pl.ds(0, TOK), lanes] = (o * lax.rsqrt(ms + epsilon) * gs[:, lanes]).astype(bf16)

    def t_send(i):
        lanes = pl.ds(pl.multiple_of(((sp + i) % HEADS) * DV, DV), DV)
        remote(tall.at[pl.ds(0, TOK), lanes], tall.at[pl.ds(TOK, TOK), lanes], t_s, t_r, partner).start()

    ph("m_w3")
    w_pass(1, 3)
    w_pass(3, 1)
    for part in range(2):
        ph(f"m_loopC{part}")

        @pl.loop(part * 4, part * 4 + 4)
        def _(i):
            attend(2 * i)

            @pl.when(i > 0)
            def _():
                t_send(2 * i - 1)

            attend(2 * i + 1)
            t_send(2 * i)

        ph(f"m_w{part + 4}")
        w_pass(2, part)
        w_pass(2, part + 2)

    ph("m_twait")
    t_send(HEADS - 1)
    loads[4].wait()
    loads[5].wait()
    remote(tall.at[pl.ds(0, TOK)], tall.at[pl.ds(TOK, TOK)], t_s, t_r, partner).wait_recv()

    def project(slot):
        acc = jnp.dot(tall[...], wall[slot], preferred_element_type=f32).astype(bf16)
        shard = ((y + 4 - slot) % 4) * 2 + c
        po[slot] = acc[TOK:]
        pj[shard] = acc[:TOK]
        remote(po.at[slot], pj.at[shard], p_s, p_r, partner).start()

    ph("m_proj0")
    project(0)
    for slot in (1, 3, 2):
        ph(f"m_ow{slot}")
        for i in range(4):
            w_wait(slot, obase + i)
        ph(f"m_proj{slot}")
        project(slot)
    ph("m_pwait")
    remote(po.at[pl.ds(0, 4)], pj.at[pl.ds(0, 4)], p_s, p_r, partner).wait_recv()

    ph("m_norm")
    total = jnp.zeros((TOK, 1), f32)
    for n in range(8):
        p = pj[n].astype(f32)
        total = total + jnp.sum(p * p, axis=-1, keepdims=True)
    r1 = lax.rsqrt(total * (1.0 / D) + epsilon)
    total = jnp.zeros((TOK, 1), f32)
    for n in range(8):
        lanes = pl.ds(n * 256, 256)
        res = (skipv[:, lanes].astype(f32) + pj[n].astype(f32) * r1 * bg[:, lanes]).astype(bf16)
        res_out[:, lanes] = res
        rs = res.astype(f32)
        total = total + jnp.sum(rs * rs, axis=-1, keepdims=True)
    r2 = lax.rsqrt(total * (1.0 / D) + epsilon)
    for j in range(16):
        lanes = pl.ds(j * 128, 128)
        rf[pl.ds(j, TOK, stride=16), :] = res_out[:, lanes].astype(f32) * r2 * pg[:, lanes]

    @pl.loop(0, 8)
    def _(i):
        x3[pl.ds(i * 16, 16)] = (
            rf[pl.ds(pl.multiple_of(i * 256, 256), 256), :].reshape(16, 16, 128).astype(bf16)
        )

    ph("e_pack")
    for one in tables:
        one.wait()

    def pack(grp):
        @pl.loop(0, PER // 4)
        def _(i):
            for u in range(4):
                o = grp * PER + i * 4 + u
                for k in range(CAP):
                    xs[o * CAP + k] = x3[jnp.clip(idx[k, o], 0, TOK - 1)]

    def send(grp, src, dst, s, r, place_of, sign):
        def one(i, to, dy):
            at = pl.ds((grp * PER + i * 4 + dy) * CAP, CAP)
            remote(src.at[at], dst.at[at], s, r.at[grp], (to, dps[(sign * dy) % 4][grp])).start()

        if grp == 0:
            pltpu.make_async_copy(src.at[pl.ds(0, CAP)], dst.at[pl.ds(0, CAP)], r.at[0]).start()

        @pl.loop(0, HEADS if grp else HEADS - 1)
        def _(j):
            i = HEADS - 1 - j
            to = place_of(i)
            for dy in (3, 2, 1, 0):
                one(i, to, dy)

        if grp == 0:
            for dy in (3, 2, 1):
                one(0, sp, dy)

    for grp in range(GROUPS):
        pack(grp)
        send(grp, xs, xr, x_s, x_r, ahead, 1)

    R = PER * CAP
    for grp in range(GROUPS):
        ph(f"e_xwait{grp}")
        at = pl.ds(grp * R, R)
        remote(xr.at[at], xr.at[at], x_s, x_r.at[grp], partner).wait_recv()
        ph(f"e_relay{grp}")

        @pl.loop(0, R // 12)
        def _(i):
            rf[pl.ds(pl.multiple_of(i * 192, 192), 192), :] = (
                xr[pl.ds(grp * R + i * 12, 12)].astype(f32).reshape(192, 128)
            )

        for j in range(16):
            xm[:, pl.ds(j * 128, 128)] = rf[pl.ds(j, R, stride=16), :].astype(bf16)
        ph(f"e_mlp{grp}")
        if grp == 0:
            experts_in[0].wait()
            experts_in[1].wait()

        @pl.loop(0, FF // 256)
        def _(n):
            lanes = pl.ds(pl.multiple_of(n * 256, 256), 256)
            a = jnp.dot(xm[...], wg[:, lanes], preferred_element_type=f32)
            b = jnp.dot(xm[...], wu[:, lanes], preferred_element_type=f32)
            hs[:, lanes] = (a * (1.0 / (1.0 + jnp.exp(-a))) * b).astype(bf16)

        if grp == 0:
            experts_in[2].wait()

        @pl.loop(0, D // 256)
        def _(n):
            lanes = pl.ds(pl.multiple_of(n * 256, 256), 256)
            a = jnp.dot(hs[...], wd[:, lanes], preferred_element_type=f32)
            rf[pl.ds(2 * n, R, stride=16), :] = a[:, :128]
            rf[pl.ds(2 * n + 1, R, stride=16), :] = a[:, 128:]

        ph(f"e_yrelay{grp}")

        @pl.loop(0, R // 12)
        def _(i):
            ys[pl.ds(grp * R + i * 12, 12)] = (
                rf[pl.ds(pl.multiple_of(i * 192, 192), 192), :].reshape(12, 16, 128).astype(bf16)
            )

        ph(f"e_ysend{grp}")
        send(grp, ys, yr, y_s, y_r, behind, -1)

    for grp in range(GROUPS):
        ph(f"e_ywait{grp}")
        at = pl.ds(grp * R, R)
        remote(yr.at[at], yr.at[at], y_s, y_r.at[grp], partner).wait_recv()

    ph("e_comb")

    @pl.loop(0, TOK // 4)
    def _(i):
        for k in range(4):
            t = i * 4 + k
            one = yr[jnp.clip(idx[CAP, t], 0, EXPERTS * CAP - 1)].astype(f32) * wts[0, t]
            two = yr[jnp.clip(idx[CAP + 1, t], 0, EXPERTS * CAP - 1)].astype(f32) * wts[1, t]
            rf[pl.ds(pl.multiple_of(t * 16, 16), 16), :] = one + two

    ph("e_norm")
    total = jnp.zeros((TOK, 1), f32)
    for j in range(16):
        p = rf[pl.ds(j, TOK, stride=16), :]
        total = total + jnp.sum(p * p, axis=-1, keepdims=True)
    r1 = lax.rsqrt(total * (1.0 / D) + epsilon)
    for j in range(16):
        lanes = pl.ds(j * 128, 128)
        norm_out[:, lanes] = rf[pl.ds(j, TOK, stride=16), :] * r1 * gain[:, lanes]

    ph("e_sendwait")
    fifteen = pl.ds(0, HEADS - 1)
    most = pl.ds(0, (EXPERTS - 1) * CAP)
    remote(spk_in.at[fifteen], spk_in.at[fifteen], spk_s, spk_r, partner).wait_send()
    remote(drecv.at[fifteen], drecv.at[fifteen], d_s, d_r, partner).wait_send()
    remote(us.at[fifteen], ur.at[fifteen], u_s, u_r.at[0, 0], partner).wait_send()
    remote(ss.at[fifteen], sr.at[fifteen], s_s, s_r.at[0, 0], partner).wait_send()
    remote(tall.at[pl.ds(0, TOK)], tall.at[pl.ds(TOK, TOK)], t_s, t_r, partner).wait_send()
    remote(po.at[pl.ds(0, 4)], pj.at[pl.ds(0, 4)], p_s, p_r, partner).wait_send()
    remote(wall.at[pl.ds(0, 3)], wall.at[pl.ds(0, 3)], w_s, w_r.at[0, 0], partner).wait_send()
    remote(xs.at[most], xr.at[most], x_s, x_r.at[0], partner).wait_send()
    remote(ys.at[most], yr.at[most], y_s, y_r.at[0], partner).wait_send()
    ph(None)


def layer(*args):
    hbm = pl.BlockSpec(memory_space=pl.ANY)
    vmem = pl.BlockSpec(memory_space=pltpu.VMEM)
    dma = pltpu.SemaphoreType.DMA
    R = PER * CAP
    return pl.pallas_call(
        layer_kernel,
        out_shape=(
            jax.ShapeDtypeStruct((TOK, D), bf16),
            jax.ShapeDtypeStruct((TOK, D), f32),
        ),
        in_specs=[hbm] * 5 + [vmem, hbm] + [vmem] * 6 + [hbm] * 3,
        out_specs=(vmem, vmem),
        scratch_shapes=[
            pltpu.VMEM((TOK, D), bf16),
            pltpu.VMEM((TOK, D), bf16),
            pltpu.VMEM((TOK, D), bf16),
            pltpu.VMEM((TOK, HEADS * DV), bf16),
            pltpu.VMEM((TOK, D), bf16),
            pltpu.VMEM((HEADS, 1, TOK), f32),
            pltpu.VMEM((4, HEADS * DV, 256), bf16),
            pltpu.VMEM((HEADS, TOK, KW), f32),
            pltpu.VMEM((HEADS, TOK, KW), bf16),
            pltpu.VMEM((HEADS, TOK, KW), bf16),
            pltpu.VMEM((HEADS, TOK, KW), bf16),
            pltpu.VMEM((HEADS, TOK, KW), bf16),
            pltpu.VMEM((HEADS, TOK, DV), f32),
            pltpu.VMEM((HEADS, DV, KW), bf16),
            pltpu.VMEM((HEADS, DV, KW), bf16),
            pltpu.VMEM((HEADS, 1, KW), f32),
            pltpu.VMEM((HEADS, 1, KW), f32),
            pltpu.VMEM((HEADS, DV, KW), bf16),
            pltpu.VMEM((HEADS, DV, KW), bf16),
            pltpu.VMEM((2 * TOK, HEADS * DV), bf16),
            pltpu.VMEM((8, TOK, 256), bf16),
            pltpu.VMEM((4, TOK, 256), bf16),
            pltpu.VMEM((R * 16, 128), f32),
            pltpu.VMEM((TOK, 16, 128), bf16),
            pltpu.VMEM((EXPERTS * CAP, 16, 128), bf16),
            pltpu.VMEM((EXPERTS * CAP, 16, 128), bf16),
            pltpu.VMEM((EXPERTS * CAP, 16, 128), bf16),
            pltpu.VMEM((EXPERTS * CAP, 16, 128), bf16),
            pltpu.VMEM((R, D), bf16),
            pltpu.VMEM((R, FF), bf16),
            pltpu.VMEM((D, FF), bf16),
            pltpu.VMEM((D, FF), bf16),
            pltpu.VMEM((FF, D), bf16),
            pltpu.VMEM((8, TOK), jnp.int32),
            pltpu.VMEM((TOP, TOK), f32),
            pltpu.SMEM((8, TOK), jnp.int32),
            pltpu.SMEM((TOP, TOK), f32),
            dma((6,)),
            dma, dma,
            dma, dma((3, 8)),
            dma, dma((2, HEADS)),
            dma, dma,
            dma, dma((2, HEADS)),
            dma, dma,
            dma, dma,
            dma((3,)), dma((2,)),
            dma, dma((GROUPS,)),
            dma, dma((GROUPS,)),
        ],
        compiler_params=pltpu.CompilerParams(
            collective_id=0, has_side_effects=True, vmem_limit_bytes=58 * 2**20
        ),
        name="layer",
    )(*args)


def shards(
    skip_stream_entering,
    mapped_probe_matrix,
    mapped_lookup_matrix,
    mapped_content_matrix,
    retention_preactivation,
    extra_shrinkage,
    attention_group_scale,
    final_projection_matrix,
    blender_branch_scale,
    specialist_prenormal_scale,
    specialist_switch_matrix,
    specialist_expand_matrix,
    specialist_contract_matrix,
    specialist_branch_scale,
    assigned_specialists,
    dispatcher_logits,
):
    res, norm = layer(
        mapped_probe_matrix[0],
        mapped_lookup_matrix[0],
        retention_preactivation[0],
        mapped_content_matrix[0],
        skip_stream_entering[0],
        extra_shrinkage[0],
        final_projection_matrix,
        attention_group_scale.reshape(1, -1),
        blender_branch_scale.reshape(1, -1),
        specialist_prenormal_scale.reshape(1, -1),
        assigned_specialists[0].T,
        dispatcher_logits[0].T,
        specialist_branch_scale.reshape(1, -1),
        specialist_switch_matrix[0],
        specialist_expand_matrix[0],
        specialist_contract_matrix[0],
    )
    return (res.astype(f32) + norm).astype(bf16)[None]


def solution(mesh):
    return jax.shard_map(
        shards,
        mesh=mesh,
        in_specs=(
            P("dp", "sp", None),
            P("dp", "sp", None),
            P("dp", "sp", None),
            P("dp", "sp", None),
            P("dp", "sp", None),
            P("dp", "sp", None),
            P(),
            P(None, "dp"),
            P(),
            P(),
            P(("sp", "dp"), None, None),
            P(("sp", "dp"), None, None),
            P(("sp", "dp"), None, None),
            P(),
            P("dp", "sp", None),
            P("dp", "sp", None),
        ),
        out_specs=P("dp", "sp", None),
        check_vma=False,
    )
```

```python
import jax
import jax.numpy as jnp
from jax import lax
from jax.experimental import pallas as pl
from jax.experimental.pallas import tpu as pltpu
from jax.sharding import PartitionSpec as P

MESH = pl.DeviceIdType.MESH
D = 2048
HEADS = 16
KW = 128
DV = 256
FF = 1024
TOK = 128
TOP = 2
CAP = 3
EXPERTS = 128
PIECE = 512
HALF = 64
GROUPS = 4
PER = EXPERTS // GROUPS

epsilon = 1e-06
f32 = jnp.float32
bf16 = jnp.bfloat16


def dot_t(a, b, ca, cb):
    return lax.dot_general(a, b, (((ca,), (cb,)), ((), ())), preferred_element_type=f32)


def phases():
    held = []

    def begin(name):
        if held:
            held.pop().__exit__(None, None, None)
        if name:
            scope = jax.named_scope(name)
            scope.__enter__()
            held.append(scope)

    return begin


def layer_kernel(
    q_h, k_h, g_h, v_h, skip_h, spk, w_h, gs, bg, pg, chosen, logits, gain, wg_h, wu_h, wd_h,
    out,
    res_v, qv, kv, gv, vv, skipv, spk_in, wall,
    bgs, lf, lw, ca, lt, intra, us, ur, dsend, drecv, ss, sr, tall, pj, po, rf,
    x3, xs, xr, ys, yr, xm, hs, wg, wu, wd, idx_v, wts_v, idx, wts,
    ready, lsem, spk_s, spk_r, w_s, w_r, u_s, u_r, d_s, d_r, s_s, s_r, t_s, t_r, p_s, p_r,
    esem, isem, x_s, x_r, y_s, y_r,
):
    ph = phases()
    sp = lax.axis_index("sp")
    dp = lax.axis_index("dp")
    z, x = sp // 4, sp % 4
    y, c = dp // 2, dp % 2
    partner = (sp, y * 2 + (1 - c))
    dps = [[((y + dy) % 4) * 2 + (c + dc) % 2 for dc in range(2)] for dy in range(4)]

    def ahead(i):
        return ((z + i // 4) % 4) * 4 + (x + i % 4) % 4

    def remote(src, dst, s, r, dev):
        return pltpu.make_async_remote_copy(
            src_ref=src, dst_ref=dst, send_sem=s, recv_sem=r, device_id=dev, device_id_type=MESH
        )

    ph("m_start")
    loads = [
        pltpu.make_async_copy(g_h, gv, lsem.at[0]),
        pltpu.make_async_copy(k_h, kv, lsem.at[1]),
        pltpu.make_async_copy(v_h, vv, lsem.at[2]),
        pltpu.make_async_copy(q_h, qv, lsem.at[3]),
        pltpu.make_async_copy(skip_h, skipv, lsem.at[4]),
        pltpu.make_async_copy(w_h, wall.at[0], lsem.at[5]),
    ]
    for one in loads:
        one.start()

    barrier = pltpu.get_barrier_semaphore()

    mates = [dps[dy][dc] for dy in range(4) for dc in range(2)][1:]
    for mate in mates:
        pl.semaphore_signal(barrier, inc=1, device_id=(sp, mate), device_id_type=MESH)

    @pl.loop(1, HEADS)
    def _(i):
        pl.semaphore_signal(
            barrier, inc=1, device_id=((sp + i) % HEADS, dp), device_id_type=MESH
        )

    row = lax.broadcasted_iota(jnp.int32, (TOK, TOK), 0)
    col = lax.broadcasted_iota(jnp.int32, (TOK, TOK), 1)
    same = (row >= col) & ((row >= HALF) == (col >= HALF))
    cross = (row >= HALF) & (col < HALF)
    first = row < HALF
    tri = jnp.where(same, 1.0, 0.0).astype(bf16)

    def split(a):
        hi = a.astype(bf16)
        rest = a - hi.astype(f32)
        mid = rest.astype(bf16)
        return hi, mid, (rest - mid.astype(f32)).astype(bf16)

    ph("m_barrier")
    pl.semaphore_wait(barrier, HEADS - 1 + len(mates))
    for mate in mates:
        pl.semaphore_signal(ready, inc=1, device_id=(sp, mate), device_id_type=MESH)
    ph("m_first")
    pltpu.make_async_copy(
        spk.at[:, pl.ds(pl.multiple_of(sp * TOK, TOK), TOK)], spk_in.at[sp], spk_r
    ).start()

    @pl.loop(1, HEADS)
    def _(i):
        to = (sp + i) % HEADS
        remote(
            spk.at[:, pl.ds(pl.multiple_of(to * TOK, TOK), TOK)], spk_in.at[sp], spk_s, spk_r, (to, dp)
        ).start()

    base = ((x + z) % 2) * 4
    obase = 4 - base
    up = (sp, dps[1][0])
    down = (sp, dps[3][0])
    around = [(ahead(1), dp), (ahead(3), dp), (ahead(4), dp), (ahead(12), dp)]

    def rows(piece):
        return pl.ds(pl.multiple_of(piece * PIECE, PIECE), PIECE)

    for i in range(4):
        a, b = base + i, base + (i + 2) % 4
        remote(w_h.at[rows(a)], wall.at[1, rows(a)], w_s, w_r.at[0, a], up).start()
        remote(w_h.at[rows(b)], wall.at[3, rows(b)], w_s, w_r.at[2, b], down).start()

    def w_wait(slot, piece):
        there = wall.at[slot, rows(piece)]
        remote(there, there, w_s, w_r.at[slot - 1, piece], partner).wait_recv()

    def w_pass(slot, i):
        piece = base + i
        w_wait(slot, piece)
        there = wall.at[slot, rows(piece)]
        if slot == 1 and i < 2:
            remote(there, wall.at[2, rows(piece)], w_s, w_r.at[1, piece], up).start()
        if slot == 3 and i >= 2:
            remote(there, wall.at[2, rows(piece)], w_s, w_r.at[1, piece], down).start()
        remote(there, there, w_s, w_r.at[slot - 1, piece], around[i]).start()

    ph("m_decay")
    loads[0].wait()

    @pl.loop(0, HEADS // 2)
    def _(i):
        for k in range(2):
            h = i * 2 + k
            g = gv[:, pl.ds(pl.multiple_of(h * KW, KW), KW)].astype(f32)
            ld = (jnp.minimum(g, 0.0) - jnp.log1p(jnp.exp(-jnp.abs(g)))) * (1.0 / 16.0)
            hi, mid, low = split(ld)
            bgs[h] = dot_t(tri, hi, 1, 0) + dot_t(tri, mid, 1, 0) + dot_t(tri, low, 1, 0)

    ph("m_route")
    esp, edp = chosen[...] >> 3, chosen[...] & 7
    off = (
        (((esp & 3) - (esp >> 2) + 8 - x + z) & 3) * 32
        + (((esp >> 2) + 4 - z) & 3) * 8
        + (((edp >> 1) + 4 - y) & 3) * 2
        + (((edp & 1) + c) & 1)
    )
    pick = [jnp.where(row == off[r : r + 1], 1.0, 0.0) for r in range(TOP)]
    named = pick[0] + pick[1]
    later = jnp.where(row < col, 1.0, 0.0).astype(bf16)
    rank = dot_t(named.astype(bf16), later, 1, 0)
    place = row.astype(f32) * CAP + rank
    idx_v[...] = jnp.zeros((8, TOK), jnp.int32)
    times = jnp.where(lax.broadcasted_iota(jnp.int32, (8, TOK), 0) >= 0, 1.0, 0.0) * (
        lax.broadcasted_iota(jnp.int32, (8, TOK), 1).astype(f32)
    )
    for k in range(CAP):
        filled = jnp.where(rank == float(k), named, 0.0).astype(bf16)
        found = dot_t(times.astype(bf16), filled, 1, 1)
        idx_v[k : k + 1, :] = jnp.minimum(found[:1], TOK - 1.0).astype(jnp.int32)
    for r in range(TOP):
        at = jnp.sum(pick[r] * place, axis=0, keepdims=True)
        idx_v[CAP + r : CAP + r + 1, :] = jnp.minimum(at, EXPERTS * CAP - 1.0).astype(jnp.int32)
    lg = logits[...]
    wts_v[...] = lg / (lg[0:1] + lg[1:2])
    tables = [
        pltpu.make_async_copy(idx_v, idx, isem.at[0]),
        pltpu.make_async_copy(wts_v, wts, isem.at[1]),
    ]

    ph("m_loadwait")
    for one in loads[1:4]:
        one.wait()
    remote(spk_in.at[pl.ds(0, HEADS)], spk_in.at[pl.ds(0, HEADS)], spk_s, spk_r, partner).wait_recv()
    ph("m_loopA")

    def u_send(h, part):
        if part == 0:
            remote(dsend.at[h], drecv.at[sp], d_s, d_r, (h, dp)).start()

        @pl.when(sp < HEADS - 1)
        def _():
            rows_u = pl.ds(part * TOK, TOK)
            remote(us.at[h, rows_u], ur.at[sp, rows_u], u_s, u_r.at[part, sp], (h, dp)).start()

    def form(h):
        lanes = pl.ds(pl.multiple_of(h * KW, KW), KW)
        hi, mid, low = split(jnp.broadcast_to(spk_in[h], (TOK, TOK)).T)
        b = bgs[h] + dot_t(tri, hi, 1, 0) + dot_t(tri, mid, 1, 0) + dot_t(tri, low, 1, 0)
        e1, e2 = b[HALF - 1 : HALF, :], b[TOK - 1 : TOK, :]
        kf = kv[:, lanes].astype(f32)
        qf = qv[:, lanes].astype(f32) * KW ** (-0.5)
        carried = kf * jnp.exp(jnp.where(first, e1, e2) - b)
        ku = carried * jnp.where(first, jnp.exp(e2), 1.0)
        vh = vv[:, pl.ds(pl.multiple_of(h * DV, DV), DV)]
        us[h] = dot_t(vh, ku.astype(bf16), 0, 0).astype(bf16)
        dsend[h] = jnp.exp(e1 + e2)
        lifted = qf * jnp.exp(b)
        lf[h] = lifted.astype(bf16)
        lw[h] = (kf * jnp.exp(-b)).astype(bf16)
        ca[h] = carried.astype(bf16)
        lt[h] = (lifted * jnp.where(first, 1.0, jnp.exp(e1))).astype(bf16)

    @pl.loop(0, HEADS // 2)
    def _(i):
        for k in range(2):
            form((sp + 1 + 2 * i + k) % HEADS)

        u_send((sp + 1 + 2 * i) % HEADS, 0)

        @pl.when(i < HEADS // 2 - 1)
        def _():
            u_send((sp + 2 + 2 * i) % HEADS, 0)

    ph("m_sendB")

    @pl.when(sp < HEADS - 1)
    def _():
        for part in range(2):
            rows_u = pl.ds(part * TOK, TOK)
            pltpu.make_async_copy(us.at[sp, rows_u], ur.at[sp, rows_u], u_r.at[part, sp]).start()

    @pl.when(sp == 0)
    def _():
        @pl.loop(0, HEADS)
        def _(i):
            sr[i] = jnp.zeros((DV, KW), bf16)

    pltpu.make_async_copy(dsend.at[sp], drecv.at[sp], d_r).start()

    @pl.loop(1, HEADS)
    def _(i):
        u_send((sp + i) % HEADS, 1)

    for one in tables:
        one.start()
    experts_in = [
        pltpu.make_async_copy(wg_h, wg, esem.at[0]),
        pltpu.make_async_copy(wu_h, wu, esem.at[1]),
        pltpu.make_async_copy(wd_h, wd, esem.at[2]),
    ]
    for one in experts_in:
        one.start()

    ph("m_loopB")

    @pl.loop(0, HEADS // 2)
    def _(i):
        for k in range(2):
            h = 2 * i + k
            vh = vv[:, pl.ds(pl.multiple_of(h * DV, DV), DV)]
            near = dot_t(lf[h], lw[h], 1, 1)
            far = dot_t(lf[h], ca[h], 1, 1)
            scores = jnp.where(same, near, jnp.where(cross, far, 0.0))
            intra[h] = dot_t(scores.astype(bf16), vh, 1, 0)

    ph("m_w0")
    w_pass(1, 0)
    w_pass(3, 2)
    ph("m_dwait")
    remote(drecv.at[pl.ds(0, HEADS)], drecv.at[pl.ds(0, HEADS)], d_s, d_r, partner).wait_recv()

    for part in range(2):
        ph(f"m_scan{part}")
        rows_u = pl.ds(part * TOK, TOK)

        def step(src, state, rows_u=rows_u, part=part):
            there = ur.at[src, rows_u]
            remote(there, there, u_s, u_r.at[part, src], partner).wait_recv()
            state = state * drecv[src] + ur[src, rows_u].astype(f32)
            to = src + 1
            ss[to, rows_u] = state.astype(bf16)

            @pl.when(to != sp)
            def _():
                remote(ss.at[to, rows_u], sr.at[sp, rows_u], s_s, s_r.at[part, sp], (to, dp)).start()

            @pl.when(to == sp)
            def _():
                pltpu.make_async_copy(ss.at[sp, rows_u], sr.at[sp, rows_u], s_r.at[part, sp]).start()

            return state

        lax.fori_loop(0, HEADS - 1, step, jnp.zeros((TOK, KW), f32))
        ph(f"m_w{part + 1}")
        w_pass(1, part + 1)
        w_pass(3, (part + 3) % 4)

    def attend(i):
        h = (sp + i) % HEADS

        @pl.when(sp > 0)
        def _():
            for part in range(2):
                there = sr.at[h, pl.ds(part * TOK, TOK)]
                remote(there, there, s_s, s_r.at[part, h], partner).wait_recv()

        o = intra[h] + dot_t(lt[h], sr[h], 1, 1)
        ms = jnp.mean(o * o, axis=-1, keepdims=True)
        lanes = pl.ds(pl.multiple_of(h * DV, DV), DV)
        tall[pl.ds(0, TOK), lanes] = (o * lax.rsqrt(ms + epsilon) * gs[:, lanes]).astype(bf16)

    def t_send(i):
        lanes = pl.ds(pl.multiple_of(((sp + i) % HEADS) * DV, DV), DV)
        remote(tall.at[pl.ds(0, TOK), lanes], tall.at[pl.ds(TOK, TOK), lanes], t_s, t_r, partner).start()

    ph("m_w3")
    w_pass(1, 3)
    w_pass(3, 1)
    for part in range(2):
        ph(f"m_w{part + 4}")
        w_pass(2, part)
        w_pass(2, part + 2)

    ph("m_loopC")

    @pl.loop(0, HEADS // 2)
    def _(i):
        attend(2 * i)

        @pl.when(i > 0)
        def _():
            t_send(2 * i - 1)

        attend(2 * i + 1)
        t_send(2 * i)

    ph("m_twait")
    t_send(HEADS - 1)
    loads[4].wait()
    loads[5].wait()
    remote(tall.at[pl.ds(0, TOK)], tall.at[pl.ds(TOK, TOK)], t_s, t_r, partner).wait_recv()

    def project(slot):
        acc = jnp.dot(tall[...], wall[slot], preferred_element_type=f32).astype(bf16)
        shard = ((y + 4 - slot) % 4) * 2 + c
        po[slot] = acc[TOK:]
        pj[shard] = acc[:TOK]
        remote(po.at[slot], pj.at[shard], p_s, p_r, partner).start()

    ph("m_proj0")
    project(0)
    for slot in (1, 3, 2):
        ph(f"m_ow{slot}")
        for i in range(4):
            w_wait(slot, obase + i)
        ph(f"m_proj{slot}")
        project(slot)
    ph("m_pwait")
    remote(po.at[pl.ds(0, 4)], pj.at[pl.ds(0, 4)], p_s, p_r, partner).wait_recv()

    ph("m_norm")
    total = jnp.zeros((TOK, 1), f32)
    for n in range(8):
        p = pj[n].astype(f32)
        total = total + jnp.sum(p * p, axis=-1, keepdims=True)
    r1 = lax.rsqrt(total * (1.0 / D) + epsilon)
    total = jnp.zeros((TOK, 1), f32)
    for n in range(8):
        lanes = pl.ds(n * 256, 256)
        res = (skipv[:, lanes].astype(f32) + pj[n].astype(f32) * r1 * bg[:, lanes]).astype(bf16)
        res_v[:, lanes] = res
        rs = res.astype(f32)
        total = total + jnp.sum(rs * rs, axis=-1, keepdims=True)
    r2 = lax.rsqrt(total * (1.0 / D) + epsilon)
    for j in range(16):
        lanes = pl.ds(j * 128, 128)
        rf[pl.ds(j, TOK, stride=16), :] = res_v[:, lanes].astype(f32) * r2 * pg[:, lanes]

    @pl.loop(0, 8)
    def _(i):
        x3[pl.ds(i * 16, 16)] = (
            rf[pl.ds(pl.multiple_of(i * 256, 256), 256), :].reshape(16, 16, 128).astype(bf16)
        )

    ph("e_pack")
    pl.semaphore_wait(ready, len(mates))
    for one in tables:
        one.wait()

    def pack(grp):
        @pl.loop(0, PER // 4)
        def _(i):
            for u in range(4):
                o = grp * PER + i * 4 + u
                for k in range(CAP):
                    xs[o * CAP + k] = x3[idx[k, o] & (TOK - 1)]

    def send(grp, src, dst, s, r, sign):
        if grp == 0:
            pltpu.make_async_copy(src.at[pl.ds(0, CAP)], dst.at[pl.ds(0, CAP)], r.at[0]).start()

        def eight(i, own):
            to = ((z + sign * i + 4) % 4) * 4 + (x + sign * (i + grp) + 8) % 4
            for dy in (2, 1, 3, 0):
                for dc in (1, 0):
                    if not (own and dy == 0 and dc == 0):
                        at = pl.ds((grp * PER + i * 8 + dy * 2 + dc) * CAP, CAP)
                        there = (to, dps[(sign * dy) % 4][dc])
                        remote(src.at[at], dst.at[at], s, r.at[grp], there).start()

        @pl.loop(0, 3 if grp == 0 else 4)
        def _(j):
            eight(3 - j, False)

        if grp == 0:
            eight(0, True)

    for grp in range(GROUPS):
        pack(grp)
        send(grp, xs, xr, x_s, x_r, 1)

    R = PER * CAP
    for grp in range(GROUPS):
        ph(f"e_xwait{grp}")
        at = pl.ds(grp * R, R)
        remote(xr.at[at], xr.at[at], x_s, x_r.at[grp], partner).wait_recv()
        ph(f"e_relay{grp}")

        @pl.loop(0, R // 12)
        def _(i):
            rf[pl.ds(pl.multiple_of(i * 192, 192), 192), :] = (
                xr[pl.ds(grp * R + i * 12, 12)].astype(f32).reshape(192, 128)
            )

        for j in range(16):
            xm[:, pl.ds(j * 128, 128)] = rf[pl.ds(j, R, stride=16), :].astype(bf16)
        ph(f"e_mlp{grp}")
        if grp == 0:
            experts_in[0].wait()
            experts_in[1].wait()

        @pl.loop(0, FF // 256)
        def _(n):
            lanes = pl.ds(pl.multiple_of(n * 256, 256), 256)
            a = jnp.dot(xm[...], wg[:, lanes], preferred_element_type=f32)
            b = jnp.dot(xm[...], wu[:, lanes], preferred_element_type=f32)
            hs[:, lanes] = (a * (1.0 / (1.0 + jnp.exp(-a))) * b).astype(bf16)

        if grp == 0:
            experts_in[2].wait()

        @pl.loop(0, D // 256)
        def _(n):
            lanes = pl.ds(pl.multiple_of(n * 256, 256), 256)
            a = jnp.dot(hs[...], wd[:, lanes], preferred_element_type=f32)
            rf[pl.ds(2 * n, R, stride=16), :] = a[:, :128]
            rf[pl.ds(2 * n + 1, R, stride=16), :] = a[:, 128:]

        ph(f"e_yrelay{grp}")

        @pl.loop(0, R // 12)
        def _(i):
            ys[pl.ds(grp * R + i * 12, 12)] = (
                rf[pl.ds(pl.multiple_of(i * 192, 192), 192), :].reshape(12, 16, 128).astype(bf16)
            )

        ph(f"e_ysend{grp}")
        send(grp, ys, yr, y_s, y_r, -1)

    for grp in range(GROUPS):
        ph(f"e_ywait{grp}")
        at = pl.ds(grp * R, R)
        remote(yr.at[at], yr.at[at], y_s, y_r.at[grp], partner).wait_recv()

    ph("e_comb")

    @pl.loop(0, TOK // 4)
    def _(i):
        for k in range(4):
            t = i * 4 + k
            one = yr[idx[CAP, t] & 511].astype(f32) * wts[0, t]
            two = yr[idx[CAP + 1, t] & 511].astype(f32) * wts[1, t]
            rf[pl.ds(pl.multiple_of(t * 16, 16), 16), :] = one + two

    ph("e_norm")
    total = jnp.zeros((TOK, 1), f32)
    for j in range(16):
        p = rf[pl.ds(j, TOK, stride=16), :]
        total = total + jnp.sum(p * p, axis=-1, keepdims=True)
    r1 = lax.rsqrt(total * (1.0 / D) + epsilon)
    for j in range(16):
        lanes = pl.ds(j * 128, 128)
        new = rf[pl.ds(j, TOK, stride=16), :] * r1 * gain[:, lanes]
        out[:, lanes] = (res_v[:, lanes].astype(f32) + new).astype(bf16)

    ph("e_sendwait")
    fifteen = pl.ds(0, HEADS - 1)
    most = pl.ds(0, (EXPERTS - 1) * CAP)
    remote(spk_in.at[fifteen], spk_in.at[fifteen], spk_s, spk_r, partner).wait_send()
    remote(drecv.at[fifteen], drecv.at[fifteen], d_s, d_r, partner).wait_send()
    @pl.when(sp < HEADS - 1)
    def _():
        remote(us.at[fifteen], ur.at[fifteen], u_s, u_r.at[0, 0], partner).wait_send()

    @pl.when(sp == 0)
    def _():
        remote(ss.at[fifteen], sr.at[fifteen], s_s, s_r.at[0, 0], partner).wait_send()

    @pl.when(sp > 0)
    def _():
        less = pl.ds(0, HEADS - 2)
        remote(ss.at[less], sr.at[less], s_s, s_r.at[0, 0], partner).wait_send()

    remote(tall.at[pl.ds(0, TOK)], tall.at[pl.ds(TOK, TOK)], t_s, t_r, partner).wait_send()
    remote(po.at[pl.ds(0, 4)], pj.at[pl.ds(0, 4)], p_s, p_r, partner).wait_send()
    remote(wall.at[pl.ds(0, 3)], wall.at[pl.ds(0, 3)], w_s, w_r.at[0, 0], partner).wait_send()
    remote(xs.at[most], xr.at[most], x_s, x_r.at[0], partner).wait_send()
    remote(ys.at[most], yr.at[most], y_s, y_r.at[0], partner).wait_send()
    ph(None)


def layer(*args):
    hbm = pl.BlockSpec(memory_space=pl.ANY)
    vmem = pl.BlockSpec(memory_space=pltpu.VMEM)
    dma = pltpu.SemaphoreType.DMA
    R = PER * CAP
    return pl.pallas_call(
        layer_kernel,
        out_shape=jax.ShapeDtypeStruct((TOK, D), bf16),
        in_specs=[hbm] * 5 + [vmem, hbm] + [vmem] * 6 + [hbm] * 3,
        out_specs=vmem,
        scratch_shapes=[
            pltpu.VMEM((TOK, D), bf16),
            pltpu.VMEM((TOK, D), bf16),
            pltpu.VMEM((TOK, D), bf16),
            pltpu.VMEM((TOK, D), bf16),
            pltpu.VMEM((TOK, HEADS * DV), bf16),
            pltpu.VMEM((TOK, D), bf16),
            pltpu.VMEM((HEADS, 1, TOK), f32),
            pltpu.VMEM((4, HEADS * DV, 256), bf16),
            pltpu.VMEM((HEADS, TOK, KW), f32),
            pltpu.VMEM((HEADS, TOK, KW), bf16),
            pltpu.VMEM((HEADS, TOK, KW), bf16),
            pltpu.VMEM((HEADS, TOK, KW), bf16),
            pltpu.VMEM((HEADS, TOK, KW), bf16),
            pltpu.VMEM((HEADS, TOK, DV), f32),
            pltpu.VMEM((HEADS, DV, KW), bf16),
            pltpu.VMEM((HEADS, DV, KW), bf16),
            pltpu.VMEM((HEADS, 1, KW), f32),
            pltpu.VMEM((HEADS, 1, KW), f32),
            pltpu.VMEM((HEADS, DV, KW), bf16),
            pltpu.VMEM((HEADS, DV, KW), bf16),
            pltpu.VMEM((2 * TOK, HEADS * DV), bf16),
            pltpu.VMEM((8, TOK, 256), bf16),
            pltpu.VMEM((4, TOK, 256), bf16),
            pltpu.VMEM((TOK * 16, 128), f32),
            pltpu.VMEM((TOK, 16, 128), bf16),
            pltpu.VMEM((EXPERTS * CAP, 16, 128), bf16),
            pltpu.VMEM((EXPERTS * CAP, 16, 128), bf16),
            pltpu.VMEM((EXPERTS * CAP, 16, 128), bf16),
            pltpu.VMEM((512, 16, 128), bf16),
            pltpu.VMEM((R, D), bf16),
            pltpu.VMEM((R, FF), bf16),
            pltpu.VMEM((D, FF), bf16),
            pltpu.VMEM((D, FF), bf16),
            pltpu.VMEM((FF, D), bf16),
            pltpu.VMEM((8, TOK), jnp.int32),
            pltpu.VMEM((TOP, TOK), f32),
            pltpu.SMEM((8, TOK), jnp.int32),
            pltpu.SMEM((TOP, TOK), f32),
            pltpu.SemaphoreType.REGULAR,
            dma((6,)),
            dma, dma,
            dma, dma((3, 8)),
            dma, dma((2, HEADS)),
            dma, dma,
            dma, dma((2, HEADS)),
            dma, dma,
            dma, dma,
            dma((3,)), dma((2,)),
            dma, dma((GROUPS,)),
            dma, dma((GROUPS,)),
        ],
        compiler_params=pltpu.CompilerParams(
            collective_id=0, has_side_effects=True, vmem_limit_bytes=58 * 2**20
        ),
        name="layer",
    )(*args)


def shards(
    skip_stream_entering,
    mapped_probe_matrix,
    mapped_lookup_matrix,
    mapped_content_matrix,
    retention_preactivation,
    extra_shrinkage,
    attention_group_scale,
    final_projection_matrix,
    blender_branch_scale,
    specialist_prenormal_scale,
    specialist_switch_matrix,
    specialist_expand_matrix,
    specialist_contract_matrix,
    specialist_branch_scale,
    assigned_specialists,
    dispatcher_logits,
):
    out = layer(
        mapped_probe_matrix[0],
        mapped_lookup_matrix[0],
        retention_preactivation[0],
        mapped_content_matrix[0],
        skip_stream_entering[0],
        extra_shrinkage[0],
        final_projection_matrix,
        attention_group_scale.reshape(1, -1),
        blender_branch_scale.reshape(1, -1),
        specialist_prenormal_scale.reshape(1, -1),
        assigned_specialists[0].T,
        dispatcher_logits[0].T,
        specialist_branch_scale.reshape(1, -1),
        specialist_switch_matrix[0],
        specialist_expand_matrix[0],
        specialist_contract_matrix[0],
    )
    return out[None]


def solution(mesh):
    return jax.shard_map(
        shards,
        mesh=mesh,
        in_specs=(
            P("dp", "sp", None),
            P("dp", "sp", None),
            P("dp", "sp", None),
            P("dp", "sp", None),
            P("dp", "sp", None),
            P("dp", "sp", None),
            P(),
            P(None, "dp"),
            P(),
            P(),
            P(("sp", "dp"), None, None),
            P(("sp", "dp"), None, None),
            P(("sp", "dp"), None, None),
            P(),
            P("dp", "sp", None),
            P("dp", "sp", None),
        ),
        out_specs=P("dp", "sp", None),
        check_vma=False,
    )
```

```python
import jax
import jax.numpy as jnp
from jax import lax
from jax.experimental import pallas as pl
from jax.experimental.pallas import tpu as pltpu
from jax.sharding import PartitionSpec as P

MESH = pl.DeviceIdType.MESH
D = 2048
HEADS = 16
KW = 128
DV = 256
FF = 1024
TOK = 128
TOP = 2
CAP = 3
EXPERTS = 128
PIECE = 512
HALF = 64
GROUPS = 2
PER = EXPERTS // GROUPS
UNROLL = 4

epsilon = 1e-06
f32 = jnp.float32
bf16 = jnp.bfloat16


def dot_t(a, b, ca, cb):
    return lax.dot_general(a, b, (((ca,), (cb,)), ((), ())), preferred_element_type=f32)


def steps_of(o):
    return [min(v, 4 - v) for v in o[:3]]


def far_first_offsets():
    every = [
        (dz, dx, dy, dc) for dz in range(4) for dx in range(4) for dy in range(4) for dc in range(2)
    ]
    return sorted(every, key=lambda o: (-sum(steps_of(o)), -o[3], steps_of(o), o))


OFFSETS = far_first_offsets()


def phases():
    held = []

    def begin(name):
        if held:
            held.pop().__exit__(None, None, None)
        if name:
            scope = jax.named_scope(name)
            scope.__enter__()
            held.append(scope)

    return begin


def layer_kernel(
    q_h, k_h, g_h, v_h, skip_h, spk, w_h, gs, bg, pg, chosen, logits, ranked, gain, wg_h, wu_h, wd_h,
    out,
    res_v, qv, kv, gv, vv, skipv, spk_in, wall,
    bgs, lf, lw, ca, lt, intra, us, ur, dsend, drecv, ss, sr, tall, pj, po, rf,
    x3, xs, xr, ys, yr, xm, hs, wg, wu, wd, idx_v, wts_v, idx, wts,
    ready, lsem, spk_s, spk_r, w_s, w_r, u_s, u_r, d_s, d_r, s_s, s_r, t_s, t_r, p_s, p_r,
    esem, isem, x_s, x_r, y_s, y_r,
):
    ph = phases()
    sp = lax.axis_index("sp")
    dp = lax.axis_index("dp")
    z, x = sp // 4, sp % 4
    y, c = dp // 2, dp % 2
    partner = (sp, y * 2 + (1 - c))
    dps = [[((y + dy) % 4) * 2 + (c + dc) % 2 for dc in range(2)] for dy in range(4)]

    def ahead(i):
        return ((z + i // 4) % 4) * 4 + (x + i % 4) % 4

    def remote(src, dst, s, r, dev):
        return pltpu.make_async_remote_copy(
            src_ref=src, dst_ref=dst, send_sem=s, recv_sem=r, device_id=dev, device_id_type=MESH
        )

    ph("m_start")
    loads = [
        pltpu.make_async_copy(g_h, gv, lsem.at[0]),
        pltpu.make_async_copy(k_h, kv, lsem.at[1]),
        pltpu.make_async_copy(v_h, vv, lsem.at[2]),
        pltpu.make_async_copy(q_h, qv, lsem.at[3]),
        pltpu.make_async_copy(skip_h, skipv, lsem.at[4]),
        pltpu.make_async_copy(w_h, wall.at[0], lsem.at[5]),
    ]
    for one in loads:
        one.start()

    barrier = pltpu.get_barrier_semaphore()

    mates = [dps[dy][dc] for dy in range(4) for dc in range(2)][1:]
    for mate in mates:
        pl.semaphore_signal(barrier, inc=1, device_id=(sp, mate), device_id_type=MESH)

    @pl.loop(1, HEADS)
    def _(i):
        pl.semaphore_signal(
            barrier, inc=1, device_id=((sp + i) % HEADS, dp), device_id_type=MESH
        )

    row = lax.broadcasted_iota(jnp.int32, (TOK, TOK), 0)
    col = lax.broadcasted_iota(jnp.int32, (TOK, TOK), 1)
    same = (row >= col) & ((row >= HALF) == (col >= HALF))
    cross = (row >= HALF) & (col < HALF)
    first = row < HALF
    tri = jnp.where(same, 1.0, 0.0).astype(bf16)

    def split(a):
        hi = a.astype(bf16)
        rest = a - hi.astype(f32)
        mid = rest.astype(bf16)
        return hi, mid, (rest - mid.astype(f32)).astype(bf16)

    ph("m_barrier")
    pl.semaphore_wait(barrier, HEADS - 1 + len(mates))
    for mate in mates:
        pl.semaphore_signal(ready, inc=1, device_id=(sp, mate), device_id_type=MESH)
    ph("m_first")
    pltpu.make_async_copy(
        spk.at[:, pl.ds(pl.multiple_of(sp * TOK, TOK), TOK)], spk_in.at[sp], spk_r
    ).start()

    @pl.loop(1, HEADS)
    def _(i):
        to = (sp + i) % HEADS
        remote(
            spk.at[:, pl.ds(pl.multiple_of(to * TOK, TOK), TOK)], spk_in.at[sp], spk_s, spk_r, (to, dp)
        ).start()

    par = (x + z) % 2
    up = (sp, dps[1][0])
    down = (sp, dps[3][0])
    around = [(ahead(1), dp), (ahead(3), dp), (ahead(4), dp), (ahead(12), dp)]

    def rows(piece):
        return pl.ds(pl.multiple_of(piece * PIECE, PIECE), PIECE)

    def mine(m):
        return par * 7 + (1 - 2 * par) * m

    def theirs(m):
        return 7 - mine(m)

    def w_up(m):
        at = rows(mine(m))
        remote(w_h.at[at], wall.at[1, at], w_s, w_r.at[0, mine(m)], up).start()

    def w_down(m):
        at = rows(mine(m))
        remote(w_h.at[at], wall.at[3, at], w_s, w_r.at[2, mine(m)], down).start()

    for m in (0, 1, 2):
        w_up(m)
    for m in (2, 3, 0):
        w_down(m)

    def w_wait(slot, piece):
        there = wall.at[slot, rows(piece)]
        remote(there, there, w_s, w_r.at[slot - 1, piece], partner).wait_recv()

    def w_share(slot, m):
        for k in range(4):
            quarter = PIECE // 4
            at = pl.ds(pl.multiple_of(mine(m) * PIECE + k * quarter, quarter), quarter)
            some = wall.at[slot, at]
            remote(some, some, w_s, w_r.at[slot - 1, mine(m)], around[k]).start()

    def w_early(m):
        for slot, n, to in ((1, m, up), (3, m + 2, down)):
            w_wait(slot, mine(n))
            at = rows(mine(n))
            remote(wall.at[slot, at], wall.at[2, at], w_s, w_r.at[1, mine(n)], to).start()
            if n < 3:
                w_share(slot, n)

    def w_pass(slot, m):
        w_wait(slot, mine(m))
        w_share(slot, m)

    ph("m_decay")
    loads[0].wait()

    @pl.loop(0, HEADS // 2)
    def _(i):
        for k in range(2):
            h = i * 2 + k
            g = gv[:, pl.ds(pl.multiple_of(h * KW, KW), KW)].astype(f32)
            ld = (jnp.minimum(g, 0.0) - jnp.log1p(jnp.exp(-jnp.abs(g)))) * (1.0 / 16.0)
            hi, mid, low = split(ld)
            bgs[h] = dot_t(tri, hi, 1, 0) + dot_t(tri, mid, 1, 0) + dot_t(tri, low, 1, 0)

    ph("m_route")
    esp, edp = chosen[...] >> 3, chosen[...] & 7
    off = (
        (((esp >> 2) + 4 - z) & 3) * 32
        + (((esp & 3) + 4 - x) & 3) * 8
        + (((edp >> 1) + 4 - y) & 3) * 2
        + (((edp & 1) + c) & 1)
    ).astype(f32)
    offset_of = jnp.broadcast_to(ranked[...], (EXPERTS, TOK)).T
    pick = [jnp.where(offset_of == off[r : r + 1], 1.0, 0.0) for r in range(TOP)]
    named = pick[0] + pick[1]
    later = jnp.where(row < col, 1.0, 0.0).astype(bf16)
    rank = dot_t(named.astype(bf16), later, 1, 0)
    place = row.astype(f32) * CAP + rank
    idx_v[...] = jnp.zeros((8, TOK), jnp.int32)
    times = jnp.where(lax.broadcasted_iota(jnp.int32, (8, TOK), 0) >= 0, 1.0, 0.0) * (
        lax.broadcasted_iota(jnp.int32, (8, TOK), 1).astype(f32)
    )
    for k in range(CAP):
        filled = jnp.where(rank == float(k), named, 0.0).astype(bf16)
        found = dot_t(times.astype(bf16), filled, 1, 1)
        idx_v[k : k + 1, :] = jnp.minimum(found[:1], TOK - 1.0).astype(jnp.int32)
    for r in range(TOP):
        at = jnp.sum(pick[r] * place, axis=0, keepdims=True)
        idx_v[CAP + r : CAP + r + 1, :] = jnp.minimum(at, EXPERTS * CAP - 1.0).astype(jnp.int32)
    lg = logits[...]
    wts_v[...] = lg / (lg[0:1] + lg[1:2])
    tables = [
        pltpu.make_async_copy(idx_v, idx, isem.at[0]),
        pltpu.make_async_copy(wts_v, wts, isem.at[1]),
    ]

    ph("m_loadwait")
    for one in loads[1:4]:
        one.wait()
    remote(spk_in.at[pl.ds(0, HEADS)], spk_in.at[pl.ds(0, HEADS)], spk_s, spk_r, partner).wait_recv()
    ph("m_loopA")

    def far_first(m):
        return (2 + m) * (1 - m // 2) + (3 - m) * (m // 2)

    def around_of(n):
        return ((z + far_first(n // 4)) % 4) * 4 + (x + far_first(n % 4)) % 4

    def u_send(h, part):
        if part == 0:
            remote(dsend.at[h], drecv.at[sp], d_s, d_r, (h, dp)).start()

        @pl.when(sp < HEADS - 1)
        def _():
            rows_u = pl.ds(part * TOK, TOK)
            remote(us.at[h, rows_u], ur.at[sp, rows_u], u_s, u_r.at[part, sp], (h, dp)).start()

    def form(h):
        lanes = pl.ds(pl.multiple_of(h * KW, KW), KW)
        hi, mid, low = split(jnp.broadcast_to(spk_in[h], (TOK, TOK)).T)
        b = bgs[h] + dot_t(tri, hi, 1, 0) + dot_t(tri, mid, 1, 0) + dot_t(tri, low, 1, 0)
        e1, e2 = b[HALF - 1 : HALF, :], b[TOK - 1 : TOK, :]
        kf = kv[:, lanes].astype(f32)
        qf = qv[:, lanes].astype(f32) * KW ** (-0.5)
        carried = kf * jnp.exp(jnp.where(first, e1, e2) - b)
        ku = carried * jnp.where(first, jnp.exp(e2), 1.0)
        vh = vv[:, pl.ds(pl.multiple_of(h * DV, DV), DV)]
        us[h] = dot_t(vh, ku.astype(bf16), 0, 0).astype(bf16)
        dsend[h] = jnp.exp(e1 + e2)
        lifted = qf * jnp.exp(b)
        lf[h] = lifted.astype(bf16)
        lw[h] = (kf * jnp.exp(-b)).astype(bf16)
        ca[h] = carried.astype(bf16)
        lt[h] = (lifted * jnp.where(first, 1.0, jnp.exp(e1))).astype(bf16)

    @pl.loop(0, HEADS // UNROLL)
    def _(i):
        for k in range(UNROLL):
            form(around_of(UNROLL * i + k))
        for k in range(UNROLL - 1):
            u_send(around_of(UNROLL * i + k), 0)

        @pl.when(i < HEADS // UNROLL - 1)
        def _():
            u_send(around_of(UNROLL * i + UNROLL - 1), 0)

    ph("m_sendB")

    @pl.when(sp < HEADS - 1)
    def _():
        for part in range(2):
            rows_u = pl.ds(part * TOK, TOK)
            pltpu.make_async_copy(us.at[sp, rows_u], ur.at[sp, rows_u], u_r.at[part, sp]).start()

    @pl.when(sp == 0)
    def _():
        @pl.loop(0, HEADS)
        def _(i):
            sr[i] = jnp.zeros((DV, KW), bf16)

    pltpu.make_async_copy(dsend.at[sp], drecv.at[sp], d_r).start()

    @pl.loop(0, HEADS - 1)
    def _(i):
        u_send(around_of(i), 1)

    for one in tables:
        one.start()
    experts_in = [
        pltpu.make_async_copy(wg_h, wg, esem.at[0]),
        pltpu.make_async_copy(wu_h, wu, esem.at[1]),
        pltpu.make_async_copy(wd_h, wd, esem.at[2]),
    ]
    for one in experts_in:
        one.start()

    ph("m_loopB")

    @pl.loop(0, HEADS // 2)
    def _(i):
        for k in range(2):
            h = 2 * i + k
            vh = vv[:, pl.ds(pl.multiple_of(h * DV, DV), DV)]
            near = dot_t(lf[h], lw[h], 1, 1)
            far = dot_t(lf[h], ca[h], 1, 1)
            scores = jnp.where(same, near, jnp.where(cross, far, 0.0))
            intra[h] = dot_t(scores.astype(bf16), vh, 1, 0)

    ph("m_w0")
    w_early(0)
    ph("m_dwait")
    remote(drecv.at[pl.ds(0, HEADS)], drecv.at[pl.ds(0, HEADS)], d_s, d_r, partner).wait_recv()

    for part in range(2):
        ph(f"m_scan{part}")
        rows_u = pl.ds(part * TOK, TOK)

        def step(src, state, rows_u=rows_u, part=part):
            there = ur.at[src, rows_u]
            remote(there, there, u_s, u_r.at[part, src], partner).wait_recv()
            state = state * drecv[src] + ur[src, rows_u].astype(f32)
            to = src + 1
            ss[to, rows_u] = state.astype(bf16)

            @pl.when(to != sp)
            def _():
                remote(ss.at[to, rows_u], sr.at[sp, rows_u], s_s, s_r.at[part, sp], (to, dp)).start()

            @pl.when(to == sp)
            def _():
                pltpu.make_async_copy(ss.at[sp, rows_u], sr.at[sp, rows_u], s_r.at[part, sp]).start()

            return state

        lax.fori_loop(0, HEADS - 1, step, jnp.zeros((TOK, KW), f32))
        ph(f"m_w{part + 1}")
        if part == 0:
            w_early(1)
            w_up(3)
            w_up(4)
            w_down(1)
            w_down(4)
        else:
            w_pass(1, 2)
            w_pass(3, 0)

    def arrived(i):
        h = (sp + i) % HEADS
        for part in range(2):
            there = sr.at[h, pl.ds(part * TOK, TOK)]
            remote(there, there, s_s, s_r.at[part, h], partner).wait_recv()

    def attend(i):
        h = (sp + i) % HEADS
        o = intra[h] + dot_t(lt[h], sr[h], 1, 1)
        ms = jnp.mean(o * o, axis=-1, keepdims=True)
        lanes = pl.ds(pl.multiple_of(h * DV, DV), DV)
        tall[pl.ds(0, TOK), lanes] = (o * lax.rsqrt(ms + epsilon) * gs[:, lanes]).astype(bf16)

    def t_send(i):
        lanes = pl.ds(pl.multiple_of(((sp + i) % HEADS) * DV, DV), DV)
        remote(tall.at[pl.ds(0, TOK), lanes], tall.at[pl.ds(TOK, TOK), lanes], t_s, t_r, partner).start()

    ph("m_w3")
    w_pass(2, 0)
    w_pass(2, 2)
    ph("m_w4")
    w_pass(2, 1)
    w_pass(2, 3)
    ph("m_w5")
    w_pass(3, 1)
    ph("m_loopC")

    @pl.loop(0, HEADS // UNROLL)
    def _(i):
        @pl.when(sp > 0)
        def _():
            for k in range(UNROLL):
                arrived(UNROLL * i + k)

        for k in range(UNROLL):
            attend(UNROLL * i + k)

        @pl.when(i > 0)
        def _():
            t_send(UNROLL * i - 1)

        for k in range(UNROLL - 1):
            t_send(UNROLL * i + k)

    ph("m_twait")
    t_send(HEADS - 1)
    loads[4].wait()
    loads[5].wait()
    remote(tall.at[pl.ds(0, TOK)], tall.at[pl.ds(TOK, TOK)], t_s, t_r, partner).wait_recv()

    def project(slot):
        acc = jnp.dot(tall[...], wall[slot], preferred_element_type=f32).astype(bf16)
        shard = ((y + 4 - slot) % 4) * 2 + c
        po[slot] = acc[TOK:]
        pj[shard] = acc[:TOK]
        remote(po.at[slot], pj.at[shard], p_s, p_r, partner).start()

    ph("m_proj0")
    project(0)
    for slot in (2, 1, 3):
        ph(f"m_ow{slot}")
        for m in range(4 if slot == 2 else 3):
            w_wait(slot, theirs(m))
        if slot == 1:
            w_wait(1, mine(3))
        if slot != 2:
            w_wait(slot, mine(4))
        ph(f"m_proj{slot}")
        project(slot)
    ph("m_pwait")
    remote(po.at[pl.ds(0, 4)], pj.at[pl.ds(0, 4)], p_s, p_r, partner).wait_recv()

    ph("m_norm")
    total = jnp.zeros((TOK, 1), f32)
    for n in range(8):
        p = pj[n].astype(f32)
        total = total + jnp.sum(p * p, axis=-1, keepdims=True)
    r1 = lax.rsqrt(total * (1.0 / D) + epsilon)
    total = jnp.zeros((TOK, 1), f32)
    for n in range(8):
        lanes = pl.ds(n * 256, 256)
        res = (skipv[:, lanes].astype(f32) + pj[n].astype(f32) * r1 * bg[:, lanes]).astype(bf16)
        res_v[:, lanes] = res
        rs = res.astype(f32)
        total = total + jnp.sum(rs * rs, axis=-1, keepdims=True)
    r2 = lax.rsqrt(total * (1.0 / D) + epsilon)
    for j in range(16):
        lanes = pl.ds(j * 128, 128)
        rf[pl.ds(j, TOK, stride=16), :] = res_v[:, lanes].astype(f32) * r2 * pg[:, lanes]

    @pl.loop(0, 8)
    def _(i):
        x3[pl.ds(i * 16, 16)] = (
            rf[pl.ds(pl.multiple_of(i * 256, 256), 256), :].reshape(16, 16, 128).astype(bf16)
        )

    ph("e_pack")
    pl.semaphore_wait(ready, len(mates))
    for one in tables:
        one.wait()

    def pack(grp):
        @pl.loop(0, PER // 4)
        def _(i):
            for u in range(4):
                o = grp * PER + i * 4 + u
                for k in range(CAP):
                    xs[o * CAP + k] = x3[idx[k, o] & (TOK - 1)]

    def send(grp, src, dst, s, r, sign):
        zs = [(z + sign * i + 4) % 4 * 4 for i in range(4)]
        xo = [(x + sign * i + 4) % 4 for i in range(4)]
        for o in range(grp * PER, grp * PER + PER):
            dz, dx, dy, dc = OFFSETS[o]
            at = pl.ds(o * CAP, CAP)
            if o < EXPERTS - 1:
                there = (zs[dz] + xo[dx], dps[(sign * dy) % 4][dc])
                remote(src.at[at], dst.at[at], s, r, there).start()
            else:
                pltpu.make_async_copy(src.at[at], dst.at[at], r).start()

    for grp in range(GROUPS):
        pack(grp)
        send(grp, xs, xr, x_s, x_r.at[grp], 1)

    R = PER * CAP
    for grp in range(GROUPS):
        low = grp * R
        ph(f"e_xwait{grp}")
        at = pl.ds(grp * R, R)
        remote(xr.at[at], xr.at[at], x_s, x_r.at[grp], partner).wait_recv()
        ph(f"e_relay{grp}")

        @pl.loop(0, R // 12)
        def _(i, low=low):
            rf[pl.ds(pl.multiple_of(i * 192, 192), 192), :] = (
                xr[pl.ds(low + i * 12, 12)].astype(f32).reshape(192, 128)
            )

        for j in range(16):
            xm[:, pl.ds(j * 128, 128)] = rf[pl.ds(j, R, stride=16), :].astype(bf16)
        ph(f"e_mlp{grp}")
        if grp == 0:
            experts_in[0].wait()
            experts_in[1].wait()

        @pl.loop(0, FF // 256)
        def _(n):
            lanes = pl.ds(pl.multiple_of(n * 256, 256), 256)
            a = jnp.dot(xm[...], wg[:, lanes], preferred_element_type=f32)
            b = jnp.dot(xm[...], wu[:, lanes], preferred_element_type=f32)
            hs[:, lanes] = (a * (1.0 / (1.0 + jnp.exp(-a))) * b).astype(bf16)

        if grp == 0:
            experts_in[2].wait()

        @pl.loop(0, D // 256)
        def _(n):
            lanes = pl.ds(pl.multiple_of(n * 256, 256), 256)
            a = jnp.dot(hs[...], wd[:, lanes], preferred_element_type=f32)
            rf[pl.ds(2 * n, R, stride=16), :] = a[:, :128]
            rf[pl.ds(2 * n + 1, R, stride=16), :] = a[:, 128:]

        ph(f"e_yrelay{grp}")

        @pl.loop(0, R // 12)
        def _(i, low=low):
            ys[pl.ds(low + i * 12, 12)] = (
                rf[pl.ds(pl.multiple_of(i * 192, 192), 192), :].reshape(12, 16, 128).astype(bf16)
            )

        ph(f"e_ysend{grp}")
        send(grp, ys, yr, y_s, y_r.at[grp], -1)

    for grp in range(GROUPS):
        ph(f"e_ywait{grp}")
        at = pl.ds(grp * R, R)
        remote(yr.at[at], yr.at[at], y_s, y_r.at[grp], partner).wait_recv()

    ph("e_comb")

    @pl.loop(0, TOK // 4)
    def _(i):
        for k in range(4):
            t = i * 4 + k
            one = yr[idx[CAP, t] & 511].astype(f32) * wts[0, t]
            two = yr[idx[CAP + 1, t] & 511].astype(f32) * wts[1, t]
            rf[pl.ds(pl.multiple_of(t * 16, 16), 16), :] = one + two

    ph("e_norm")
    total = jnp.zeros((TOK, 1), f32)
    for j in range(16):
        p = rf[pl.ds(j, TOK, stride=16), :]
        total = total + jnp.sum(p * p, axis=-1, keepdims=True)
    r1 = lax.rsqrt(total * (1.0 / D) + epsilon)
    for j in range(16):
        lanes = pl.ds(j * 128, 128)
        new = rf[pl.ds(j, TOK, stride=16), :] * r1 * gain[:, lanes]
        out[:, lanes] = (res_v[:, lanes].astype(f32) + new).astype(bf16)

    ph("e_sendwait")
    fifteen = pl.ds(0, HEADS - 1)
    most = pl.ds(0, (EXPERTS - 1) * CAP)
    remote(spk_in.at[fifteen], spk_in.at[fifteen], spk_s, spk_r, partner).wait_send()
    remote(drecv.at[fifteen], drecv.at[fifteen], d_s, d_r, partner).wait_send()
    @pl.when(sp < HEADS - 1)
    def _():
        remote(us.at[fifteen], ur.at[fifteen], u_s, u_r.at[0, 0], partner).wait_send()

    @pl.when(sp == 0)
    def _():
        remote(ss.at[fifteen], sr.at[fifteen], s_s, s_r.at[0, 0], partner).wait_send()

    @pl.when(sp > 0)
    def _():
        less = pl.ds(0, HEADS - 2)
        remote(ss.at[less], sr.at[less], s_s, s_r.at[0, 0], partner).wait_send()

    remote(tall.at[pl.ds(0, TOK)], tall.at[pl.ds(TOK, TOK)], t_s, t_r, partner).wait_send()
    remote(po.at[pl.ds(0, 4)], pj.at[pl.ds(0, 4)], p_s, p_r, partner).wait_send()
    remote(wall.at[pl.ds(0, 3)], wall.at[pl.ds(0, 3)], w_s, w_r.at[0, 0], partner).wait_send()
    remote(xs.at[most], xr.at[most], x_s, x_r.at[0], partner).wait_send()
    remote(ys.at[most], yr.at[most], y_s, y_r.at[0], partner).wait_send()
    ph(None)


def layer(*args):
    hbm = pl.BlockSpec(memory_space=pl.ANY)
    vmem = pl.BlockSpec(memory_space=pltpu.VMEM)
    dma = pltpu.SemaphoreType.DMA
    R = PER * CAP
    return pl.pallas_call(
        layer_kernel,
        out_shape=jax.ShapeDtypeStruct((TOK, D), bf16),
        in_specs=[hbm] * 5 + [vmem, hbm] + [vmem] * 7 + [hbm] * 3,
        out_specs=vmem,
        scratch_shapes=[
            pltpu.VMEM((TOK, D), bf16),
            pltpu.VMEM((TOK, D), bf16),
            pltpu.VMEM((TOK, D), bf16),
            pltpu.VMEM((TOK, D), bf16),
            pltpu.VMEM((TOK, HEADS * DV), bf16),
            pltpu.VMEM((TOK, D), bf16),
            pltpu.VMEM((HEADS, 1, TOK), f32),
            pltpu.VMEM((4, HEADS * DV, 256), bf16),
            pltpu.VMEM((HEADS, TOK, KW), f32),
            pltpu.VMEM((HEADS, TOK, KW), bf16),
            pltpu.VMEM((HEADS, TOK, KW), bf16),
            pltpu.VMEM((HEADS, TOK, KW), bf16),
            pltpu.VMEM((HEADS, TOK, KW), bf16),
            pltpu.VMEM((HEADS, TOK, DV), f32),
            pltpu.VMEM((HEADS, DV, KW), bf16),
            pltpu.VMEM((HEADS, DV, KW), bf16),
            pltpu.VMEM((HEADS, 1, KW), f32),
            pltpu.VMEM((HEADS, 1, KW), f32),
            pltpu.VMEM((HEADS, DV, KW), bf16),
            pltpu.VMEM((HEADS, DV, KW), bf16),
            pltpu.VMEM((2 * TOK, HEADS * DV), bf16),
            pltpu.VMEM((8, TOK, 256), bf16),
            pltpu.VMEM((4, TOK, 256), bf16),
            pltpu.VMEM((R * 16, 128), f32),
            pltpu.VMEM((TOK, 16, 128), bf16),
            pltpu.VMEM((EXPERTS * CAP, 16, 128), bf16),
            pltpu.VMEM((EXPERTS * CAP, 16, 128), bf16),
            pltpu.VMEM((EXPERTS * CAP, 16, 128), bf16),
            pltpu.VMEM((512, 16, 128), bf16),
            pltpu.VMEM((R, D), bf16),
            pltpu.VMEM((R, FF), bf16),
            pltpu.VMEM((D, FF), bf16),
            pltpu.VMEM((D, FF), bf16),
            pltpu.VMEM((FF, D), bf16),
            pltpu.VMEM((8, TOK), jnp.int32),
            pltpu.VMEM((TOP, TOK), f32),
            pltpu.SMEM((8, TOK), jnp.int32),
            pltpu.SMEM((TOP, TOK), f32),
            pltpu.SemaphoreType.REGULAR,
            dma((6,)),
            dma, dma,
            dma, dma((3, 8)),
            dma, dma((2, HEADS)),
            dma, dma,
            dma, dma((2, HEADS)),
            dma, dma,
            dma, dma,
            dma((3,)), dma((2,)),
            dma, dma((GROUPS,)),
            dma, dma((GROUPS,)),
        ],
        compiler_params=pltpu.CompilerParams(
            collective_id=0, has_side_effects=True, vmem_limit_bytes=58 * 2**20
        ),
        name="layer",
    )(*args)


def shards(
    skip_stream_entering,
    mapped_probe_matrix,
    mapped_lookup_matrix,
    mapped_content_matrix,
    retention_preactivation,
    extra_shrinkage,
    attention_group_scale,
    final_projection_matrix,
    blender_branch_scale,
    specialist_prenormal_scale,
    specialist_switch_matrix,
    specialist_expand_matrix,
    specialist_contract_matrix,
    specialist_branch_scale,
    assigned_specialists,
    dispatcher_logits,
):
    out = layer(
        mapped_probe_matrix[0],
        mapped_lookup_matrix[0],
        retention_preactivation[0],
        mapped_content_matrix[0],
        skip_stream_entering[0],
        extra_shrinkage[0],
        final_projection_matrix,
        attention_group_scale.reshape(1, -1),
        blender_branch_scale.reshape(1, -1),
        specialist_prenormal_scale.reshape(1, -1),
        assigned_specialists[0].T,
        dispatcher_logits[0].T,
        jnp.array([[dz * 32 + dx * 8 + dy * 2 + dc for dz, dx, dy, dc in OFFSETS]], f32),
        specialist_branch_scale.reshape(1, -1),
        specialist_switch_matrix[0],
        specialist_expand_matrix[0],
        specialist_contract_matrix[0],
    )
    return out[None]


def solution(mesh):
    return jax.shard_map(
        shards,
        mesh=mesh,
        in_specs=(
            P("dp", "sp", None),
            P("dp", "sp", None),
            P("dp", "sp", None),
            P("dp", "sp", None),
            P("dp", "sp", None),
            P("dp", "sp", None),
            P(),
            P(None, "dp"),
            P(),
            P(),
            P(("sp", "dp"), None, None),
            P(("sp", "dp"), None, None),
            P(("sp", "dp"), None, None),
            P(),
            P("dp", "sp", None),
            P("dp", "sp", None),
        ),
        out_specs=P("dp", "sp", None),
        check_vma=False,
    )
```

```python
import jax
import jax.numpy as jnp
from jax import lax
from jax.experimental import pallas as pl
from jax.experimental.pallas import tpu as pltpu
from jax.sharding import PartitionSpec as P

MESH = pl.DeviceIdType.MESH
D = 2048
HEADS = 16
KW = 128
DV = 256
FF = 1024
TOK = 128
TOP = 2
CAP = 3
EXPERTS = 128
PIECE = 512
HALF = 64
SIZES = (32, 48, 48)
ORDER = (1, 3, 2)
LAST = (1, 3, 2)
UNROLL = 4

epsilon = 1e-06
f32 = jnp.float32
bf16 = jnp.bfloat16


def dot_t(a, b, ca, cb):
    return lax.dot_general(a, b, (((ca,), (cb,)), ((), ())), preferred_element_type=f32)


def steps_of(o):
    return [min(v, 4 - v) for v in o[:3]]


def far_first_offsets():
    every = [
        (dz, dx, dy, dc) for dz in range(4) for dx in range(4) for dy in range(4) for dc in range(2)
    ]
    return sorted(every, key=lambda o: (-sum(steps_of(o)), -o[3], steps_of(o), o))


OFFSETS = far_first_offsets()


def phases():
    held = []

    def begin(name):
        if held:
            held.pop().__exit__(None, None, None)
        if name:
            scope = jax.named_scope(name)
            scope.__enter__()
            held.append(scope)

    return begin


def layer_kernel(
    q_h, k_h, g_h, v_h, skip_h, spk, w_h, gs, bg, pg, chosen, logits, ranked, gain, wg_h, wu_h, wd_h,
    out,
    res_v, qv, kv, gv, vv, skipv, spk_in, wall,
    bgs, lf, lw, ca, lt, intra, us, ur, dsend, drecv, ss, sr, tall, pj, po, rf,
    part_sum, x3, xs, xr, ys, yr, xm, hs, wg, wu, wd, idx_v, wts_v, idx, wts,
    ready, lsem, spk_s, spk_r, w_s, w_r, u_s, u_r, d_s, d_r, s_s, s_r, t_s, t_r, p_s, p_r,
    esem, isem, x_s, x_r, y_s, y_r,
):
    ph = phases()
    sp = lax.axis_index("sp")
    dp = lax.axis_index("dp")
    z, x = sp // 4, sp % 4
    y, c = dp // 2, dp % 2
    partner = (sp, y * 2 + (1 - c))
    dps = [[((y + dy) % 4) * 2 + (c + dc) % 2 for dc in range(2)] for dy in range(4)]

    def ahead(i):
        return ((z + i // 4) % 4) * 4 + (x + i % 4) % 4

    def remote(src, dst, s, r, dev):
        return pltpu.make_async_remote_copy(
            src_ref=src, dst_ref=dst, send_sem=s, recv_sem=r, device_id=dev, device_id_type=MESH
        )

    ph("m_start")
    loads = [
        pltpu.make_async_copy(g_h, gv, lsem.at[0]),
        pltpu.make_async_copy(k_h, kv, lsem.at[1]),
        pltpu.make_async_copy(v_h, vv, lsem.at[2]),
        pltpu.make_async_copy(q_h, qv, lsem.at[3]),
        pltpu.make_async_copy(skip_h, skipv, lsem.at[4]),
        pltpu.make_async_copy(w_h, wall.at[0], lsem.at[5]),
    ]
    for one in loads:
        one.start()

    barrier = pltpu.get_barrier_semaphore()

    mates = [dps[dy][dc] for dy in range(4) for dc in range(2)][1:]
    for mate in mates:
        pl.semaphore_signal(barrier, inc=1, device_id=(sp, mate), device_id_type=MESH)

    @pl.loop(1, HEADS)
    def _(i):
        pl.semaphore_signal(
            barrier, inc=1, device_id=((sp + i) % HEADS, dp), device_id_type=MESH
        )

    row = lax.broadcasted_iota(jnp.int32, (TOK, TOK), 0)
    col = lax.broadcasted_iota(jnp.int32, (TOK, TOK), 1)
    same = (row >= col) & ((row >= HALF) == (col >= HALF))
    cross = (row >= HALF) & (col < HALF)
    first = row < HALF
    tri = jnp.where(same, 1.0, 0.0).astype(bf16)

    def split(a):
        hi = a.astype(bf16)
        rest = a - hi.astype(f32)
        mid = rest.astype(bf16)
        return hi, mid, (rest - mid.astype(f32)).astype(bf16)

    ph("m_barrier")
    pl.semaphore_wait(barrier, HEADS - 1 + len(mates))
    for mate in mates:
        pl.semaphore_signal(ready, inc=1, device_id=(sp, mate), device_id_type=MESH)
    ph("m_first")
    pltpu.make_async_copy(
        spk.at[:, pl.ds(pl.multiple_of(sp * TOK, TOK), TOK)], spk_in.at[sp], spk_r
    ).start()

    @pl.loop(1, HEADS)
    def _(i):
        to = (sp + i) % HEADS
        remote(
            spk.at[:, pl.ds(pl.multiple_of(to * TOK, TOK), TOK)], spk_in.at[sp], spk_s, spk_r, (to, dp)
        ).start()

    par = (x + z) % 2
    up = (sp, dps[1][0])
    down = (sp, dps[3][0])
    around = [(ahead(1), dp), (ahead(3), dp), (ahead(4), dp), (ahead(12), dp)]

    def rows(piece):
        return pl.ds(pl.multiple_of(piece * PIECE, PIECE), PIECE)

    def mine(m):
        return par * 7 + (1 - 2 * par) * m

    def theirs(m):
        return 7 - mine(m)

    def w_up(m):
        at = rows(mine(m))
        remote(w_h.at[at], wall.at[1, at], w_s, w_r.at[0, mine(m)], up).start()

    def w_down(m):
        at = rows(mine(m))
        remote(w_h.at[at], wall.at[3, at], w_s, w_r.at[2, mine(m)], down).start()

    for m in (0, 1, 2):
        w_up(m)
    for m in (2, 3, 0):
        w_down(m)

    def w_wait(slot, piece):
        there = wall.at[slot, rows(piece)]
        remote(there, there, w_s, w_r.at[slot - 1, piece], partner).wait_recv()

    def w_share(slot, m):
        for k in range(4):
            quarter = PIECE // 4
            at = pl.ds(pl.multiple_of(mine(m) * PIECE + k * quarter, quarter), quarter)
            some = wall.at[slot, at]
            remote(some, some, w_s, w_r.at[slot - 1, mine(m)], around[k]).start()

    def w_early(m):
        for slot, n, to in ((1, m, up), (3, m + 2, down)):
            w_wait(slot, mine(n))
            at = rows(mine(n))
            remote(wall.at[slot, at], wall.at[2, at], w_s, w_r.at[1, mine(n)], to).start()
            if n < 3:
                w_share(slot, n)

    def w_pass(slot, m):
        w_wait(slot, mine(m))
        w_share(slot, m)

    ph("m_decay")
    loads[0].wait()

    @pl.loop(0, HEADS // 2)
    def _(i):
        for k in range(2):
            h = i * 2 + k
            g = gv[:, pl.ds(pl.multiple_of(h * KW, KW), KW)].astype(f32)
            ld = (jnp.minimum(g, 0.0) - jnp.log1p(jnp.exp(-jnp.abs(g)))) * (1.0 / 16.0)
            hi, mid, low = split(ld)
            bgs[h] = dot_t(tri, hi, 1, 0) + dot_t(tri, mid, 1, 0) + dot_t(tri, low, 1, 0)

    ph("m_route")
    esp, edp = chosen[...] >> 3, chosen[...] & 7
    off = (
        (((esp >> 2) + 4 - z) & 3) * 32
        + (((esp & 3) + 4 - x) & 3) * 8
        + (((edp >> 1) + 4 - y) & 3) * 2
        + (((edp & 1) + c) & 1)
    ).astype(f32)
    offset_of = jnp.broadcast_to(ranked[...], (EXPERTS, TOK)).T
    pick = [jnp.where(offset_of == off[r : r + 1], 1.0, 0.0) for r in range(TOP)]
    named = pick[0] + pick[1]
    later = jnp.where(row < col, 1.0, 0.0).astype(bf16)
    rank = dot_t(named.astype(bf16), later, 1, 0)
    place = row.astype(f32) * CAP + rank
    idx_v[...] = jnp.zeros((8, TOK), jnp.int32)
    times = jnp.where(lax.broadcasted_iota(jnp.int32, (8, TOK), 0) >= 0, 1.0, 0.0) * (
        lax.broadcasted_iota(jnp.int32, (8, TOK), 1).astype(f32)
    )
    for k in range(CAP):
        filled = jnp.where(rank == float(k), named, 0.0).astype(bf16)
        found = dot_t(times.astype(bf16), filled, 1, 1)
        idx_v[k : k + 1, :] = jnp.minimum(found[:1], TOK - 1.0).astype(jnp.int32)
    for r in range(TOP):
        at = jnp.sum(pick[r] * place, axis=0, keepdims=True)
        idx_v[CAP + r : CAP + r + 1, :] = jnp.minimum(at, EXPERTS * CAP - 1.0).astype(jnp.int32)
    lg = logits[...]
    wts_v[...] = lg / (lg[0:1] + lg[1:2])
    tables = [
        pltpu.make_async_copy(idx_v, idx, isem.at[0]),
        pltpu.make_async_copy(wts_v, wts, isem.at[1]),
    ]

    ph("m_loadwait")
    for one in loads[1:4]:
        one.wait()
    remote(spk_in.at[pl.ds(0, HEADS)], spk_in.at[pl.ds(0, HEADS)], spk_s, spk_r, partner).wait_recv()
    ph("m_loopA")

    def far_first(m):
        return (2 + m) * (1 - m // 2) + (3 - m) * (m // 2)

    def around_of(n):
        return ((z + far_first(n // 4)) % 4) * 4 + (x + far_first(n % 4)) % 4

    def u_send(h, part):
        if part == 0:
            remote(dsend.at[h], drecv.at[sp], d_s, d_r, (h, dp)).start()

        @pl.when(sp < HEADS - 1)
        def _():
            rows_u = pl.ds(part * TOK, TOK)
            remote(us.at[h, rows_u], ur.at[sp, rows_u], u_s, u_r.at[part, sp], (h, dp)).start()

    def form(h):
        lanes = pl.ds(pl.multiple_of(h * KW, KW), KW)
        hi, mid, low = split(jnp.broadcast_to(spk_in[h], (TOK, TOK)).T)
        b = bgs[h] + dot_t(tri, hi, 1, 0) + dot_t(tri, mid, 1, 0) + dot_t(tri, low, 1, 0)
        e1, e2 = b[HALF - 1 : HALF, :], b[TOK - 1 : TOK, :]
        kf = kv[:, lanes].astype(f32)
        qf = qv[:, lanes].astype(f32) * KW ** (-0.5)
        carried = kf * jnp.exp(jnp.where(first, e1, e2) - b)
        ku = carried * jnp.where(first, jnp.exp(e2), 1.0)
        vh = vv[:, pl.ds(pl.multiple_of(h * DV, DV), DV)]
        us[h] = dot_t(vh, ku.astype(bf16), 0, 0).astype(bf16)
        dsend[h] = jnp.exp(e1 + e2)
        lifted = qf * jnp.exp(b)
        lf[h] = lifted.astype(bf16)
        lw[h] = (kf * jnp.exp(-b)).astype(bf16)
        ca[h] = carried.astype(bf16)
        lt[h] = (lifted * jnp.where(first, 1.0, jnp.exp(e1))).astype(bf16)

    @pl.loop(0, HEADS // UNROLL)
    def _(i):
        for k in range(UNROLL):
            form(around_of(UNROLL * i + k))
        for k in range(UNROLL - 1):
            u_send(around_of(UNROLL * i + k), 0)

        @pl.when(i < HEADS // UNROLL - 1)
        def _():
            u_send(around_of(UNROLL * i + UNROLL - 1), 0)

    ph("m_sendB")

    @pl.when(sp < HEADS - 1)
    def _():
        for part in range(2):
            rows_u = pl.ds(part * TOK, TOK)
            pltpu.make_async_copy(us.at[sp, rows_u], ur.at[sp, rows_u], u_r.at[part, sp]).start()

    @pl.when(sp == 0)
    def _():
        @pl.loop(0, HEADS)
        def _(i):
            sr[i] = jnp.zeros((DV, KW), bf16)

    pltpu.make_async_copy(dsend.at[sp], drecv.at[sp], d_r).start()

    @pl.loop(0, HEADS - 1)
    def _(i):
        u_send(around_of(i), 1)

    for one in tables:
        one.start()
    experts_in = [
        pltpu.make_async_copy(wg_h, wg, esem.at[0]),
        pltpu.make_async_copy(wu_h, wu, esem.at[1]),
        pltpu.make_async_copy(wd_h, wd, esem.at[2]),
    ]
    for one in experts_in:
        one.start()

    ph("m_loopB")

    @pl.loop(0, HEADS // 2)
    def _(i):
        for k in range(2):
            h = 2 * i + k
            vh = vv[:, pl.ds(pl.multiple_of(h * DV, DV), DV)]
            near = dot_t(lf[h], lw[h], 1, 1)
            far = dot_t(lf[h], ca[h], 1, 1)
            scores = jnp.where(same, near, jnp.where(cross, far, 0.0))
            intra[h] = dot_t(scores.astype(bf16), vh, 1, 0)

    ph("m_w0")
    w_early(0)
    ph("m_dwait")
    remote(drecv.at[pl.ds(0, HEADS)], drecv.at[pl.ds(0, HEADS)], d_s, d_r, partner).wait_recv()

    for part in range(2):
        ph(f"m_scan{part}")
        rows_u = pl.ds(part * TOK, TOK)

        def step(src, state, rows_u=rows_u, part=part):
            there = ur.at[src, rows_u]
            remote(there, there, u_s, u_r.at[part, src], partner).wait_recv()
            state = state * drecv[src] + ur[src, rows_u].astype(f32)
            to = src + 1
            ss[to, rows_u] = state.astype(bf16)

            @pl.when(to != sp)
            def _():
                remote(ss.at[to, rows_u], sr.at[sp, rows_u], s_s, s_r.at[part, sp], (to, dp)).start()

            @pl.when(to == sp)
            def _():
                pltpu.make_async_copy(ss.at[sp, rows_u], sr.at[sp, rows_u], s_r.at[part, sp]).start()

            return state

        lax.fori_loop(0, HEADS - 1, step, jnp.zeros((TOK, KW), f32))
        ph(f"m_w{part + 1}")
        if part == 0:
            w_early(1)
            w_up(3)
            w_up(4)
            w_down(1)
            w_down(4)
        else:
            w_pass(1, 2)
            w_pass(3, 0)

    def arrived(i):
        h = (sp + i) % HEADS
        for part in range(2):
            there = sr.at[h, pl.ds(part * TOK, TOK)]
            remote(there, there, s_s, s_r.at[part, h], partner).wait_recv()

    def attend(i):
        h = (sp + i) % HEADS
        o = intra[h] + dot_t(lt[h], sr[h], 1, 1)
        ms = jnp.mean(o * o, axis=-1, keepdims=True)
        lanes = pl.ds(pl.multiple_of(h * DV, DV), DV)
        tall[pl.ds(0, TOK), lanes] = (o * lax.rsqrt(ms + epsilon) * gs[:, lanes]).astype(bf16)

    def t_send(i):
        lanes = pl.ds(pl.multiple_of(((sp + i) % HEADS) * DV, DV), DV)
        remote(tall.at[pl.ds(0, TOK), lanes], tall.at[pl.ds(TOK, TOK), lanes], t_s, t_r, partner).start()

    ph("m_w3")
    w_pass(2, 0)
    w_pass(2, 2)
    ph("m_w4")
    w_pass(2, 1)
    w_pass(2, 3)
    ph("m_loopC")

    @pl.loop(0, HEADS // UNROLL)
    def _(i):
        @pl.when(sp > 0)
        def _():
            for k in range(UNROLL):
                arrived(UNROLL * i + k)

        for k in range(UNROLL):
            attend(UNROLL * i + k)

        @pl.when(i > 0)
        def _():
            t_send(UNROLL * i - 1)

        for k in range(UNROLL - 1):
            t_send(UNROLL * i + k)

    ph("m_w5")
    w_pass(3, 1)
    ph("m_twait")
    t_send(HEADS - 1)
    loads[4].wait()
    loads[5].wait()
    remote(tall.at[pl.ds(0, TOK)], tall.at[pl.ds(TOK, TOK)], t_s, t_r, partner).wait_recv()

    def pieces_dot(slot, pieces):
        total = None
        for piece in pieces:
            at = rows(piece)
            term = jnp.dot(tall[:, at], wall[slot, at], preferred_element_type=f32)
            total = term if total is None else total + term
        return total

    def hand_out(slot, acc):
        acc = acc.astype(bf16)
        shard = ((y + 4 - slot) % 4) * 2 + c
        po[slot] = acc[TOK:]
        pj[shard] = acc[:TOK]
        remote(po.at[slot], pj.at[shard], p_s, p_r, partner).start()

    ph("m_proj0")
    hand_out(0, jnp.dot(tall[...], wall[0], preferred_element_type=f32))
    late = {1: [mine(4)], 2: [theirs(1), theirs(3)], 3: [mine(4), theirs(1)]}
    soon = {
        1: [mine(0), mine(1), mine(2), mine(3), theirs(0), theirs(1), theirs(2)],
        2: [mine(0), mine(1), mine(2), mine(3), theirs(0), theirs(2)],
        3: [mine(0), mine(1), mine(2), mine(3), theirs(0), theirs(2)],
    }
    waits = {
        1: [mine(3), theirs(0), theirs(1), theirs(2)],
        2: [theirs(0), theirs(2)],
        3: [theirs(0), theirs(2)],
    }
    for slot in ORDER:
        ph(f"m_ow{slot}")
        for piece in waits[slot]:
            w_wait(slot, piece)
        ph(f"m_proj{slot}")
        part_sum[slot - 1] = pieces_dot(slot, soon[slot])
    for slot in LAST:
        ph(f"m_lw{slot}")
        for piece in late[slot]:
            w_wait(slot, piece)
        ph(f"m_last{slot}")
        hand_out(slot, part_sum[slot - 1] + pieces_dot(slot, late[slot]))
    ph("m_pwait")
    remote(po.at[pl.ds(0, 4)], pj.at[pl.ds(0, 4)], p_s, p_r, partner).wait_recv()

    ph("m_norm")
    total = jnp.zeros((TOK, 1), f32)
    for n in range(8):
        p = pj[n].astype(f32)
        total = total + jnp.sum(p * p, axis=-1, keepdims=True)
    r1 = lax.rsqrt(total * (1.0 / D) + epsilon)
    total = jnp.zeros((TOK, 1), f32)
    for n in range(8):
        lanes = pl.ds(n * 256, 256)
        res = (skipv[:, lanes].astype(f32) + pj[n].astype(f32) * r1 * bg[:, lanes]).astype(bf16)
        res_v[:, lanes] = res
        rs = res.astype(f32)
        total = total + jnp.sum(rs * rs, axis=-1, keepdims=True)
    r2 = lax.rsqrt(total * (1.0 / D) + epsilon)
    for j in range(16):
        lanes = pl.ds(j * 128, 128)
        rf[pl.ds(j, TOK, stride=16), :] = res_v[:, lanes].astype(f32) * r2 * pg[:, lanes]

    @pl.loop(0, 8)
    def _(i):
        x3[pl.ds(i * 16, 16)] = (
            rf[pl.ds(pl.multiple_of(i * 256, 256), 256), :].reshape(16, 16, 128).astype(bf16)
        )

    ph("e_pack")
    pl.semaphore_wait(ready, len(mates))
    for one in tables:
        one.wait()

    first = [sum(SIZES[:grp]) for grp in range(len(SIZES))]

    def span(grp):
        return pl.ds(first[grp] * CAP, SIZES[grp] * CAP)

    def pack(grp):
        @pl.loop(0, SIZES[grp] // 4)
        def _(i):
            for u in range(4):
                o = first[grp] + i * 4 + u
                for k in range(CAP):
                    xs[o * CAP + k] = x3[idx[k, o] & (TOK - 1)]

    def send(grp, src, dst, s, r, sign):
        zs = [(z + sign * i + 4) % 4 * 4 for i in range(4)]
        xo = [(x + sign * i + 4) % 4 for i in range(4)]
        for o in range(first[grp], first[grp] + SIZES[grp]):
            dz, dx, dy, dc = OFFSETS[o]
            at = pl.ds(o * CAP, CAP)
            if o < EXPERTS - 1:
                there = (zs[dz] + xo[dx], dps[(sign * dy) % 4][dc])
                remote(src.at[at], dst.at[at], s, r, there).start()
            else:
                pltpu.make_async_copy(src.at[at], dst.at[at], r).start()

    for grp in range(len(SIZES)):
        pack(grp)
        send(grp, xs, xr, x_s, x_r.at[grp], 1)

    for grp in range(len(SIZES)):
        R = SIZES[grp] * CAP
        low = first[grp] * CAP
        ph(f"e_xwait{grp}")
        at = span(grp)
        remote(xr.at[at], xr.at[at], x_s, x_r.at[grp], partner).wait_recv()
        ph(f"e_relay{grp}")

        @pl.loop(0, R // 12)
        def _(i, low=low):
            rf[pl.ds(pl.multiple_of(i * 192, 192), 192), :] = (
                xr[pl.ds(low + i * 12, 12)].astype(f32).reshape(192, 128)
            )

        for j in range(16):
            xm[pl.ds(0, R), pl.ds(j * 128, 128)] = rf[pl.ds(j, R, stride=16), :].astype(bf16)
        ph(f"e_mlp{grp}")
        if grp == 0:
            experts_in[0].wait()
            experts_in[1].wait()

        @pl.loop(0, FF // 256)
        def _(n, R=R):
            lanes = pl.ds(pl.multiple_of(n * 256, 256), 256)
            a = jnp.dot(xm[pl.ds(0, R), :], wg[:, lanes], preferred_element_type=f32)
            b = jnp.dot(xm[pl.ds(0, R), :], wu[:, lanes], preferred_element_type=f32)
            hs[pl.ds(0, R), lanes] = (a * (1.0 / (1.0 + jnp.exp(-a))) * b).astype(bf16)

        if grp == 0:
            experts_in[2].wait()

        @pl.loop(0, D // 256)
        def _(n, R=R):
            lanes = pl.ds(pl.multiple_of(n * 256, 256), 256)
            a = jnp.dot(hs[pl.ds(0, R), :], wd[:, lanes], preferred_element_type=f32)
            rf[pl.ds(2 * n, R, stride=16), :] = a[:, :128]
            rf[pl.ds(2 * n + 1, R, stride=16), :] = a[:, 128:]

        ph(f"e_yrelay{grp}")

        @pl.loop(0, R // 12)
        def _(i, low=low):
            ys[pl.ds(low + i * 12, 12)] = (
                rf[pl.ds(pl.multiple_of(i * 192, 192), 192), :].reshape(12, 16, 128).astype(bf16)
            )

        ph(f"e_ysend{grp}")
        send(grp, ys, yr, y_s, y_r.at[grp], -1)

    for grp in range(len(SIZES)):
        ph(f"e_ywait{grp}")
        at = span(grp)
        remote(yr.at[at], yr.at[at], y_s, y_r.at[grp], partner).wait_recv()

    ph("e_comb")

    @pl.loop(0, TOK // 4)
    def _(i):
        for k in range(4):
            t = i * 4 + k
            one = yr[idx[CAP, t] & 511].astype(f32) * wts[0, t]
            two = yr[idx[CAP + 1, t] & 511].astype(f32) * wts[1, t]
            rf[pl.ds(pl.multiple_of(t * 16, 16), 16), :] = one + two

    ph("e_norm")
    total = jnp.zeros((TOK, 1), f32)
    for j in range(16):
        p = rf[pl.ds(j, TOK, stride=16), :]
        total = total + jnp.sum(p * p, axis=-1, keepdims=True)
    r1 = lax.rsqrt(total * (1.0 / D) + epsilon)
    for j in range(16):
        lanes = pl.ds(j * 128, 128)
        new = rf[pl.ds(j, TOK, stride=16), :] * r1 * gain[:, lanes]
        out[:, lanes] = (res_v[:, lanes].astype(f32) + new).astype(bf16)

    ph("e_sendwait")
    fifteen = pl.ds(0, HEADS - 1)
    most = pl.ds(0, (EXPERTS - 1) * CAP)
    remote(spk_in.at[fifteen], spk_in.at[fifteen], spk_s, spk_r, partner).wait_send()
    remote(drecv.at[fifteen], drecv.at[fifteen], d_s, d_r, partner).wait_send()
    @pl.when(sp < HEADS - 1)
    def _():
        remote(us.at[fifteen], ur.at[fifteen], u_s, u_r.at[0, 0], partner).wait_send()

    @pl.when(sp == 0)
    def _():
        remote(ss.at[fifteen], sr.at[fifteen], s_s, s_r.at[0, 0], partner).wait_send()

    @pl.when(sp > 0)
    def _():
        less = pl.ds(0, HEADS - 2)
        remote(ss.at[less], sr.at[less], s_s, s_r.at[0, 0], partner).wait_send()

    remote(tall.at[pl.ds(0, TOK)], tall.at[pl.ds(TOK, TOK)], t_s, t_r, partner).wait_send()
    remote(po.at[pl.ds(0, 4)], pj.at[pl.ds(0, 4)], p_s, p_r, partner).wait_send()
    remote(wall.at[pl.ds(0, 3)], wall.at[pl.ds(0, 3)], w_s, w_r.at[0, 0], partner).wait_send()
    remote(xs.at[most], xr.at[most], x_s, x_r.at[0], partner).wait_send()
    remote(ys.at[most], yr.at[most], y_s, y_r.at[0], partner).wait_send()
    ph(None)


def layer(*args):
    hbm = pl.BlockSpec(memory_space=pl.ANY)
    vmem = pl.BlockSpec(memory_space=pltpu.VMEM)
    dma = pltpu.SemaphoreType.DMA
    R = max(SIZES) * CAP
    return pl.pallas_call(
        layer_kernel,
        out_shape=jax.ShapeDtypeStruct((TOK, D), bf16),
        in_specs=[hbm] * 5 + [vmem, hbm] + [vmem] * 7 + [hbm] * 3,
        out_specs=vmem,
        scratch_shapes=[
            pltpu.VMEM((TOK, D), bf16),
            pltpu.VMEM((TOK, D), bf16),
            pltpu.VMEM((TOK, D), bf16),
            pltpu.VMEM((TOK, D), bf16),
            pltpu.VMEM((TOK, HEADS * DV), bf16),
            pltpu.VMEM((TOK, D), bf16),
            pltpu.VMEM((HEADS, 1, TOK), f32),
            pltpu.VMEM((4, HEADS * DV, 256), bf16),
            pltpu.VMEM((HEADS, TOK, KW), f32),
            pltpu.VMEM((HEADS, TOK, KW), bf16),
            pltpu.VMEM((HEADS, TOK, KW), bf16),
            pltpu.VMEM((HEADS, TOK, KW), bf16),
            pltpu.VMEM((HEADS, TOK, KW), bf16),
            pltpu.VMEM((HEADS, TOK, DV), f32),
            pltpu.VMEM((HEADS, DV, KW), bf16),
            pltpu.VMEM((HEADS, DV, KW), bf16),
            pltpu.VMEM((HEADS, 1, KW), f32),
            pltpu.VMEM((HEADS, 1, KW), f32),
            pltpu.VMEM((HEADS, DV, KW), bf16),
            pltpu.VMEM((HEADS, DV, KW), bf16),
            pltpu.VMEM((2 * TOK, HEADS * DV), bf16),
            pltpu.VMEM((8, TOK, 256), bf16),
            pltpu.VMEM((4, TOK, 256), bf16),
            pltpu.VMEM((R * 16, 128), f32),
            pltpu.VMEM((3, 2 * TOK, 256), f32),
            pltpu.VMEM((TOK, 16, 128), bf16),
            pltpu.VMEM((EXPERTS * CAP, 16, 128), bf16),
            pltpu.VMEM((EXPERTS * CAP, 16, 128), bf16),
            pltpu.VMEM((EXPERTS * CAP, 16, 128), bf16),
            pltpu.VMEM((512, 16, 128), bf16),
            pltpu.VMEM((R, D), bf16),
            pltpu.VMEM((R, FF), bf16),
            pltpu.VMEM((D, FF), bf16),
            pltpu.VMEM((D, FF), bf16),
            pltpu.VMEM((FF, D), bf16),
            pltpu.VMEM((8, TOK), jnp.int32),
            pltpu.VMEM((TOP, TOK), f32),
            pltpu.SMEM((8, TOK), jnp.int32),
            pltpu.SMEM((TOP, TOK), f32),
            pltpu.SemaphoreType.REGULAR,
            dma((6,)),
            dma, dma,
            dma, dma((3, 8)),
            dma, dma((2, HEADS)),
            dma, dma,
            dma, dma((2, HEADS)),
            dma, dma,
            dma, dma,
            dma((3,)), dma((2,)),
            dma, dma((len(SIZES),)),
            dma, dma((len(SIZES),)),
        ],
        compiler_params=pltpu.CompilerParams(
            collective_id=0, has_side_effects=True, vmem_limit_bytes=58 * 2**20
        ),
        name="layer",
    )(*args)


def shards(
    skip_stream_entering,
    mapped_probe_matrix,
    mapped_lookup_matrix,
    mapped_content_matrix,
    retention_preactivation,
    extra_shrinkage,
    attention_group_scale,
    final_projection_matrix,
    blender_branch_scale,
    specialist_prenormal_scale,
    specialist_switch_matrix,
    specialist_expand_matrix,
    specialist_contract_matrix,
    specialist_branch_scale,
    assigned_specialists,
    dispatcher_logits,
):
    out = layer(
        mapped_probe_matrix[0],
        mapped_lookup_matrix[0],
        retention_preactivation[0],
        mapped_content_matrix[0],
        skip_stream_entering[0],
        extra_shrinkage[0],
        final_projection_matrix,
        attention_group_scale.reshape(1, -1),
        blender_branch_scale.reshape(1, -1),
        specialist_prenormal_scale.reshape(1, -1),
        assigned_specialists[0].T,
        dispatcher_logits[0].T,
        jnp.array([[dz * 32 + dx * 8 + dy * 2 + dc for dz, dx, dy, dc in OFFSETS]], f32),
        specialist_branch_scale.reshape(1, -1),
        specialist_switch_matrix[0],
        specialist_expand_matrix[0],
        specialist_contract_matrix[0],
    )
    return out[None]


def solution(mesh):
    return jax.shard_map(
        shards,
        mesh=mesh,
        in_specs=(
            P("dp", "sp", None),
            P("dp", "sp", None),
            P("dp", "sp", None),
            P("dp", "sp", None),
            P("dp", "sp", None),
            P("dp", "sp", None),
            P(),
            P(None, "dp"),
            P(),
            P(),
            P(("sp", "dp"), None, None),
            P(("sp", "dp"), None, None),
            P(("sp", "dp"), None, None),
            P(),
            P("dp", "sp", None),
            P("dp", "sp", None),
        ),
        out_specs=P("dp", "sp", None),
        check_vma=False,
    )
```
